32 devices in a mesh: sp: 8 (over z, x), tp: 4 (over y, core).
Axes of the slice: x: 2, y: 2, z: 4, core: 2. Of those that a mesh axis runs over, the one named last changes fastest.
Arguments:
- tokens: bfloat16 [3072, 2048], P('sp'), may hold values from -6 to 6
- doc_ids: int32 [3072], P('sp'), may hold values from 0 to 2, never falling along the last dimension, each value on 1 to 2048 neighbouring positions
- pre_gain: float32 [2, 2048], replicated, may hold values from 0.1 to 1.9
- value_proj: bfloat16 [2, 2048, 1024], P(None, 'sp', 'tp'), may hold values from -0.1875 to 0.1875
- gate_proj: bfloat16 [2, 2048, 1024], P(None, 'sp', 'tp'), may hold values from -0.1875 to 0.1875
- out_proj: bfloat16 [2, 1024, 2048], P(None, 'tp', 'sp'), may hold values from -0.1875 to 0.1875
- conv_taps: float32 [2, 31, 1024], P(None, None, 'tp'), may hold values from -2.2 to 2.2
- norm_gain: float32 [2, 1024], P(None, 'tp'), may hold values from 0.1 to 1.9
- norm_shift: float32 [2, 1024], P(None, 'tp'), may hold values from -3 to 3
Outputs:
- hidden: bfloat16 [3072, 2048], P('sp')
The draws below stay inside these ranges and needn't reach their ends.
Inputs may be any that keep to these rules, and one draw needn't show every extreme that they name: `doc_ids`: document numbers never fall along the sequence; each document has 1 to 2048 positions.
All inputs are finite; a program needn't handle non-finite values.
Results may differ from the reference program's by a relative error of at most 0.017.
Values may be sent and summed in bfloat16 or wider, within the bound.
No kernel may reach another device: no remote copies, remote signals or barrier semaphores. Data moves between devices by JAX's collectives and lax.ppermute only.
A program may use at most 64 MiB of HBM per device.

```python
import math
import jax
import jax.numpy as jnp
import numpy as np
from jax import lax

D = 2048
C = 1024
KW = 31
LAYERS = 2
TOKENS = 3072
DOCS = 3
DOC_MOST = 2048
N_TP = 4


def draw_conv_taps(key, part):
    scale_key = jax.random.fold_in(key, 11)
    tap_key = jax.random.fold_in(key, 12)
    group_scale = jnp.exp(jax.random.uniform(scale_key, (8,), jnp.float32, jnp.log(0.25), jnp.log(4.0)))
    channel_scale = jnp.repeat(group_scale, C // 8)
    raw = jnp.clip(jax.random.normal(tap_key, (LAYERS, KW, C), jnp.float32), -3.0, 3.0)
    return raw * channel_scale[None, None, :] / jnp.sqrt(jnp.float32(KW))


def spiked(drawn, stream_key, source, target, parts, factor):
    owner, partner = [(jnp.arange(drawn.shape[dim]) // (drawn.shape[dim] // parts)).reshape([-1 if axis == dim else 1 for axis in range(drawn.ndim)]) for dim in (source, target)]
    chosen = jax.random.permutation(stream_key, parts)[partner]
    strong = (owner == chosen) | (owner == (partner + parts // 2) % parts)
    return jnp.where(strong, factor * drawn, drawn)


def levels(rng, dims, shards, smallest, high):
    factor_of, own = 1.0, jax.random.fold_in(rng, 6)
    for dim, parts in shards:
        heights = jnp.exp(jax.random.uniform(jax.random.fold_in(own, dim), (parts,), jnp.float32, smallest / len(shards), high / len(shards)))
        factor_of = factor_of * jnp.repeat(heights, dims[dim] // parts).reshape([-1 if axis == dim else 1 for axis in range(len(dims))])
    return factor_of


def length_profile(count, total, most, lean):
    portions = [(1 << 20) // math.isqrt(rank ** lean) + 1 for rank in range(2, count + 1)]
    rest, holding = total - most - (count - 1), [1] * (count - 1)
    while rest > 0:
        movable = [i for i in range(count - 1) if holding[i] < most]
        whole, remaining = sum([portions[i] for i in movable]), rest
        for i in movable:
            extra = min(most - holding[i], max(1, remaining * portions[i] // whole), rest)
            holding[i] = holding[i] + extra
            rest = rest - extra
    return np.array([most] + holding)


def ragged_sizes(own_key, number_of, total, limit, slope):
    if number_of == 2:
        one = jax.random.randint(own_key, (), max(1, total - limit), min(limit, total - 1) + 1)
        return jnp.stack([one, total - one])
    sizes = jnp.asarray(length_profile(number_of, total, limit, slope), jnp.int32)
    couples = (number_of - 1) // 2
    giver, receiver = sizes[1:1 + 2 * couples:2], sizes[2:2 + 2 * couples:2]
    margin = jnp.minimum(giver - 1, limit - receiver)
    passed = jax.random.randint(jax.random.fold_in(own_key, 1), (couples,), 0, 1 << 20) % (margin + 1)
    sizes = sizes.at[1:1 + 2 * couples:2].set(giver - passed).at[2:2 + 2 * couples:2].set(receiver + passed)
    return sizes[jax.random.permutation(jax.random.fold_in(own_key, 2), number_of)]


def scatter_about(rng, extent, scale, most, cuts=(), held_as=jnp.bfloat16):
    array = scale * jax.random.normal(rng, extent, jnp.float32)
    if cuts:
        array = array * levels(rng, extent, cuts, -0.22, 0.18)
    return jnp.clip(array, -most, most).astype(held_as)


def gaussian_with(rng, dims, scale, limit, cuts, heavy, dtype=jnp.bfloat16):
    array = scale * jax.random.normal(rng, dims, jnp.float32)
    if cuts:
        array = array * levels(rng, dims, cuts, -0.22, 0.18)
    return jnp.clip(spiked(array, jax.random.fold_in(rng, 3), *heavy), -limit, limit).astype(dtype)


def setup_inputs(seed: int = 0) -> dict:
    seeds = jax.random.split(jax.random.key(seed), 10)
    tokens = scatter_about(seeds[0], (TOKENS, D), 1.0, 6.0, ((0, 8),))
    doc_ids = jnp.searchsorted(jnp.cumsum(ragged_sizes(seeds[1], DOCS, TOKENS, DOC_MOST, 0)), jnp.arange(TOKENS), side="right").astype(jnp.int32)
    pre_gain = jnp.clip(1.0 + 0.18 * jax.random.normal(seeds[2], (LAYERS, D), jnp.float32), 0.1, 1.9)
    value_proj = gaussian_with(seeds[3], (LAYERS, D, C), D ** -0.5, 0.1875, ((1, 8), (2, 4)), (1, 2, 8, 2.0))
    gate_proj = gaussian_with(seeds[4], (LAYERS, D, C), D ** -0.5, 0.1875, ((1, 8), (2, 4)), (1, 2, 8, 2.0))
    out_proj = scatter_about(seeds[5], (LAYERS, C, D), C ** -0.5, 0.1875, ((1, 4), (2, 8)))
    conv_taps = draw_conv_taps(jax.random.fold_in(seeds[9], 71), 0)
    norm_gain = jnp.clip(1.0 + 0.18 * jax.random.normal(seeds[7], (LAYERS, C), jnp.float32), 0.1, 1.9)
    norm_shift = scatter_about(seeds[8], (LAYERS, C), 0.5, 3.0, ((1, 4),), jnp.float32)
    return dict(tokens=tokens, doc_ids=doc_ids, pre_gain=pre_gain, value_proj=value_proj, gate_proj=gate_proj, out_proj=out_proj, conv_taps=conv_taps, norm_gain=norm_gain, norm_shift=norm_shift)


epsilon = 1e-06

def reference(tokens, doc_ids, pre_gain, value_proj, gate_proj, out_proj, conv_taps, norm_gain, norm_shift):
    hidden = tokens
    padded_docs = jnp.concatenate([jnp.full((KW - 1,), -1, jnp.int32), doc_ids.astype(jnp.int32)])
    block_width = C // N_TP
    for layer_index in range(LAYERS):
        wide_state = hidden.astype(jnp.float32)
        scale = lax.rsqrt(lax.optimization_barrier(jnp.mean(wide_state * wide_state, axis=-1, keepdims=True)) + epsilon)
        normed = (wide_state * scale * pre_gain[layer_index]).astype(jnp.bfloat16)
        value_half = jnp.dot(normed, value_proj[layer_index], preferred_element_type=jnp.float32).astype(jnp.bfloat16)
        gate_half = jnp.dot(normed, gate_proj[layer_index], preferred_element_type=jnp.float32).astype(jnp.bfloat16)
        gated_rows = (value_half.astype(jnp.float32) * jax.nn.sigmoid(gate_half.astype(jnp.float32))).astype(jnp.bfloat16)
        padded = jnp.concatenate([jnp.zeros((KW - 1, C), jnp.bfloat16), gated_rows]).astype(jnp.float32)
        conv_out = jnp.zeros((TOKENS, C), jnp.float32)
        for offset in range(KW):
            first_row = KW - 1 - offset
            same_doc = (padded_docs[first_row:first_row + TOKENS] == doc_ids)[:, None]
            term = conv_taps[layer_index, offset][None, :] * padded[first_row:first_row + TOKENS]
            conv_out = conv_out + jnp.where(same_doc, term, jnp.float32(0.0))
        row_mean = lax.optimization_barrier(jnp.mean(conv_out, axis=-1, keepdims=True))
        row_var = lax.optimization_barrier(jnp.mean(jnp.square(conv_out - row_mean), axis=-1, keepdims=True))
        normalized = norm_gain[layer_index] * (conv_out - row_mean) * lax.rsqrt(row_var + epsilon) + norm_shift[layer_index]
        activated = jax.nn.silu(normalized).astype(jnp.bfloat16)
        total = jnp.zeros((TOKENS, D), jnp.float32)
        for block_index in range(N_TP):
            lower = block_index * block_width
            share = jnp.dot(activated[:, lower:lower + block_width], out_proj[layer_index, lower:lower + block_width], preferred_element_type=jnp.float32)
            total = total + share.astype(jnp.bfloat16).astype(jnp.float32)
        branch = total.astype(jnp.bfloat16)
        hidden = (hidden.astype(jnp.float32) + branch.astype(jnp.float32)).astype(jnp.bfloat16)
    return hidden
```

```python
import functools

import jax
import jax.numpy as jnp
from jax import lax
from jax.experimental import pallas as pl
from jax.experimental.pallas import tpu as pltpu
from jax.sharding import PartitionSpec as P

epsilon = 1e-06
LANES = 128
SUBLANES = 8
HALO_ALIGN = 16
CONV_ROWS = 32
RING_MOST = 16


wide = jnp.float32
narrow = jnp.bfloat16


def round_up(value, step):
    return -(-value // step) * step


def in_vmem():
    return pl.BlockSpec(memory_space=pltpu.VMEM)


def in_smem():
    return pl.BlockSpec(memory_space=pltpu.SMEM)


def normed_of(state, gain):
    scale = lax.rsqrt(jnp.mean(state * state, axis=-1, keepdims=True) + epsilon)
    return (state * scale * gain).astype(narrow)


def norm_body(state_ref, gain_ref, normed_ref):
    normed_ref[...] = normed_of(state_ref[...].astype(wide), gain_ref[...])


def gated_conv_body(
    tap_count, tail, place_ref, normed_ref, dist_ref, taps_ref, *refs
):
    *chunk_refs, centred_ref, stats_ref, acc_ref, shifted_ref, conv_ref = refs
    width = taps_ref.shape[1]
    halves = width // LANES
    rows = normed_ref.shape[0]
    out_rows = centred_ref.shape[0]
    depth = chunk_refs[0].shape[0]
    for k, chunk in enumerate(chunk_refs):
        first = pl.multiple_of(place_ref[k] * depth, LANES)
        product = jnp.dot(
            normed_ref[:, pl.ds(first, depth)], chunk[...], preferred_element_type=wide
        )
        if k == 0:
            acc_ref[...] = product
        else:
            acc_ref[...] += product
    for half in range(halves):
        cols = slice(half * LANES, (half + 1) * LANES)
        gate_cols = slice(width + half * LANES, width + (half + 1) * LANES)
        value = acc_ref[:, cols].astype(narrow).astype(wide)
        gate = acc_ref[:, gate_cols].astype(narrow).astype(wide)
        gated = (value * jax.nn.sigmoid(gate)).astype(narrow).astype(wide)
        shifted_ref[half, 0, :, :] = gated
    for half in range(halves):
        for shift in range(1, SUBLANES):
            shifted_ref[half, shift, SUBLANES:, :] = shifted_ref[
                half, 0, SUBLANES - shift : rows - shift, :
            ]

    def block(index, carry):
        base = index * CONV_ROWS
        dist = dist_ref[pl.ds(pl.multiple_of(base, CONV_ROWS), CONV_ROWS), :]
        sums = [jnp.zeros((CONV_ROWS, LANES), wide) for _ in range(halves)]
        for tap in range(tap_count):
            inside = dist >= tap
            start = pl.multiple_of(base + (tail - tap // SUBLANES * SUBLANES), SUBLANES)
            for half in range(halves):
                rows_at = shifted_ref[half, tap % SUBLANES, pl.ds(start, CONV_ROWS), :]
                weight = taps_ref[tap : tap + 1, half * LANES : (half + 1) * LANES]
                sums[half] = sums[half] + jnp.where(inside, weight * rows_at, 0.0)
        for half in range(halves):
            conv_ref[half, pl.ds(pl.multiple_of(base, CONV_ROWS), CONV_ROWS), :] = sums[half]
        return carry

    lax.fori_loop(0, out_rows // CONV_ROWS, block, 0)
    total = conv_ref[0]
    for half in range(1, halves):
        total = total + conv_ref[half]
    mean = jnp.sum(total, axis=1, keepdims=True) / width
    square = jnp.zeros((out_rows, LANES), wide)
    for half in range(halves):
        centred = conv_ref[half] - mean
        centred_ref[:, half * LANES : (half + 1) * LANES] = centred.astype(narrow)
        square = square + centred * centred
    square = jnp.sum(square, axis=1, keepdims=True)
    lane = lax.broadcasted_iota(jnp.int32, (out_rows, LANES), 1)
    both = jnp.where(lane == 0, mean, square)
    padded_rows = stats_ref.shape[1]
    if padded_rows != out_rows:
        both = jnp.concatenate([both, jnp.zeros((padded_rows - out_rows, LANES), wide)])
    stats_ref[...] = both.T[:2, :]


def project_body(
    block_width, tp_count, place_ref, blocks_ref, stats_ref, gain_ref, shift_ref, *refs
):
    *in_refs, share_ref, act_ref = refs
    far_count = gain_ref.shape[0]
    centred_refs, chunk_refs = in_refs[:far_count], in_refs[far_count:]
    out_rows, width = centred_refs[0].shape
    stats = stats_ref[...].T[:out_rows, :]
    means = [stats[:, 2 * j : 2 * j + 1] for j in range(tp_count)]
    mean = functools.reduce(jnp.add, means) / tp_count
    square = sum(
        stats[:, 2 * j + 1 : 2 * j + 2] + width * (means[j] - mean) ** 2 for j in range(tp_count)
    )
    scale = lax.rsqrt(square / (width * tp_count) + epsilon)
    for f, centred in enumerate(centred_refs):
        own = jnp.zeros_like(mean)
        for j in range(tp_count):
            own = jnp.where(blocks_ref[f] == j, means[j], own)
        offset = own - mean
        gain = gain_ref[f : f + 1, :]
        shift = shift_ref[f : f + 1, :]
        normal = gain * (centred[...].astype(wide) + offset) * scale + shift
        act_ref[f] = (normal * jax.nn.sigmoid(normal)).astype(narrow)
    for k, chunk in enumerate(chunk_refs):
        share = jnp.dot(act_ref[0], chunk[0], preferred_element_type=wide)
        for f in range(1, far_count):
            share = share + jnp.dot(act_ref[f], chunk[f], preferred_element_type=wide)
        cols = chunk.shape[2]
        first = pl.multiple_of(place_ref[k] * cols, LANES)
        share_ref[:, pl.ds(first, cols)] = share.astype(narrow)


def add_body(skip, with_norm, state_ref, *refs):
    if with_norm:
        gain_ref, *share_refs, hidden_ref, normed_ref = refs
    else:
        *share_refs, hidden_ref = refs
    branch = share_refs[0][...].astype(wide)
    for share in share_refs[1:]:
        branch = branch + share[...].astype(wide)
    hidden = (
        state_ref[skip:, :].astype(wide) + branch.astype(narrow).astype(wide)
    ).astype(narrow)
    hidden_ref[...] = hidden
    if with_norm:
        normed_ref[...] = normed_of(hidden.astype(wide), gain_ref[...])


def ring_tables(count):
    order = list(range(0, count, 2)) + list(range(count - 1, 0, -2))
    forward = [(order[k], order[(k + 1) % count]) for k in range(count)]
    backward = [(target, source) for source, target in forward]
    steps = [0]
    for k in range(1, count // 2 + 1):
        steps.append(-k)
        if len(steps) < count:
            steps.append(k)
    position = {device: k for k, device in enumerate(order)}
    table = [[order[(position[s] + step) % count] for step in steps] for s in range(count)]
    return forward, backward, table


def ring_gathered(value, axis):
    count = lax.axis_size(axis)
    forward, backward, _ = ring_tables(count)
    chunks = [value]
    ahead = behind = value
    for _ in range(count // 2):
        ahead = lax.ppermute(ahead, axis, forward)
        chunks.append(ahead)
        if len(chunks) < count:
            behind = lax.ppermute(behind, axis, backward)
            chunks.append(behind)
    return chunks


def gathered(value, axis, dim):
    count = lax.axis_size(axis)
    if count <= RING_MOST and count % 2 == 0 and value.shape[dim] % LANES == 0:
        return ring_gathered(value, axis)
    return [lax.all_gather(value, axis, axis=dim, tiled=True)]


def places(axis, chunk_count):
    if chunk_count == 1:
        return jnp.zeros((1,), jnp.int32)
    table = jnp.asarray(ring_tables(lax.axis_size(axis))[2], jnp.int32)
    return lax.dynamic_index_in_dim(table, lax.axis_index(axis), keepdims=False)


def swapped(value, axis, group, step):
    count = lax.axis_size(axis)
    pairs = []
    for source in range(count):
        lead, at = source // (group * step), source // step % group
        for other in range(group):
            if (at + 1) % group == other:
                target = lead * group * step + other * step + source % step
                pairs.append((source, target))
    return lax.ppermute(value, axis, pairs)


def on_device(
    tokens, doc_ids, pre_gain, value_proj, gate_proj, out_proj, conv_taps, norm_gain, norm_shift
):
    layer_count = value_proj.shape[0]
    tap_count = conv_taps.shape[1]
    row_count, model_width = tokens.shape
    width = conv_taps.shape[2]
    sp_count, tp_count = lax.axis_size("sp"), lax.axis_size("tp")
    near = 2 if tp_count % 2 == 0 else 1
    far = tp_count // near
    tail = round_up(tap_count - 1, max(HALO_ALIGN, CONV_ROWS))
    halo = tail * layer_count

    pair_proj = [
        jnp.concatenate([value_proj[n], gate_proj[n]], axis=1) for n in range(layer_count)
    ]
    pair_chunks = [None] * layer_count
    out_chunks = [None] * layer_count
    far_out = [out_proj]
    far_norm = [jnp.stack([norm_gain, norm_shift])]
    for _ in range(1, far):
        far_out.append(swapped(far_out[-1], "tp", far, near))
        far_norm.append(swapped(far_norm[-1], "tp", far, near))
    for n in range(layer_count):
        pair_chunks[n] = gathered(pair_proj[n], "sp", 0)
        out_chunks[n] = gathered(jnp.stack([part[n] for part in far_out]), "sp", 2)

    onward = [(source, source + 1) for source in range(sp_count - 1)]
    prev_rows = lax.ppermute(tokens[row_count - halo :], "sp", onward)
    prev_docs = lax.ppermute(doc_ids[row_count - halo :] + 1, "sp", onward) - 1
    state = jnp.concatenate([prev_rows, tokens])
    docs = jnp.concatenate([prev_docs, doc_ids])
    dist = jnp.zeros((row_count + halo - tail,), jnp.int32)
    for offset in range(1, tap_count):
        first = tail - offset
        dist = dist + (docs[first : first + dist.shape[0]] == docs[tail:]).astype(jnp.int32)
    dist = jnp.broadcast_to(dist[:, None], (dist.shape[0], LANES))

    tp_index = lax.axis_index("tp")
    lead, at = tp_index // near // far, tp_index // near % far
    blocks = jnp.stack(
        [(lead * far + (at - f) % far) * near + tp_index % near for f in range(far)]
    ).astype(jnp.int32)

    normed = pl.pallas_call(
        norm_body,
        out_shape=jax.ShapeDtypeStruct(state.shape, narrow),
        in_specs=[in_vmem(), in_vmem()],
        out_specs=in_vmem(),
    )(state, pre_gain[0][None, :])

    for n in range(layer_count):
        rows = state.shape[0]
        out_rows = rows - tail
        padded = round_up(out_rows, LANES)
        chunks = pair_chunks[n]
        centred, stats = pl.pallas_call(
            functools.partial(gated_conv_body, tap_count, tail),
            out_shape=(
                jax.ShapeDtypeStruct((out_rows, width), narrow),
                jax.ShapeDtypeStruct((2, padded), wide),
            ),
            in_specs=[in_smem()] + [in_vmem()] * (3 + len(chunks)),
            out_specs=(in_vmem(), in_vmem()),
            scratch_shapes=[
                pltpu.VMEM((rows, 2 * width), wide),
                pltpu.VMEM((width // LANES, SUBLANES, rows, LANES), wide),
                pltpu.VMEM((width // LANES, out_rows, LANES), wide),
            ],
        )(
            places("sp", len(chunks)),
            normed,
            dist[dist.shape[0] - out_rows :],
            conv_taps[n],
            *chunks,
        )
        far_centred = [centred]
        for _ in range(1, far):
            far_centred.append(swapped(far_centred[-1], "tp", far, near))
        all_stats = lax.all_gather(stats, "tp", axis=0, tiled=True)
        chunks = out_chunks[n]
        share = pl.pallas_call(
            functools.partial(project_body, width, tp_count),
            out_shape=jax.ShapeDtypeStruct((out_rows, model_width), narrow),
            in_specs=[in_smem(), in_smem()] + [in_vmem()] * (3 + far + len(chunks)),
            out_specs=in_vmem(),
            scratch_shapes=[pltpu.VMEM((far, out_rows, width), narrow)],
        )(
            places("sp", len(chunks)),
            blocks,
            all_stats,
            jnp.stack([part[0, n] for part in far_norm]),
            jnp.stack([part[1, n] for part in far_norm]),
            *far_centred,
            *chunks,
        )
        shares = [share]
        for _ in range(1, near):
            shares.append(swapped(shares[-1], "tp", near, 1))
        last = n == layer_count - 1
        shape = jax.ShapeDtypeStruct((out_rows, model_width), narrow)
        extra = () if last else (pre_gain[n + 1][None, :],)
        result = pl.pallas_call(
            functools.partial(add_body, tail, not last),
            out_shape=shape if last else (shape, shape),
            in_specs=[in_vmem()] * (1 + len(extra) + len(shares)),
            out_specs=in_vmem() if last else (in_vmem(), in_vmem()),
        )(state, *extra, *shares)
        state, normed = (result, None) if last else result
    return state


def solution(mesh):
    return jax.shard_map(
        on_device,
        mesh=mesh,
        in_specs=(
            P("sp", None),
            P("sp"),
            P(),
            P(None, "sp", "tp"),
            P(None, "sp", "tp"),
            P(None, "tp", "sp"),
            P(None, None, "tp"),
            P(None, "tp"),
            P(None, "tp"),
        ),
        out_specs=P("sp", None),
        check_vma=False,
    )
```

```python
import functools

import jax
import jax.numpy as jnp
from jax import lax
from jax.experimental import pallas as pl
from jax.experimental.pallas import tpu as pltpu
from jax.sharding import PartitionSpec as P


epsilon = 1e-06
LANES = 128
SUBLANES = 8
HALO_ALIGN = 16
CONV_ROWS = 32
RING_MOST = 8
KERNEL_VMEM = 20 * 2**20


wide = jnp.float32
narrow = jnp.bfloat16


def round_up(value, step):
    return -(-value // step) * step


def in_vmem():
    return pl.BlockSpec(memory_space=pltpu.VMEM)


def in_smem():
    return pl.BlockSpec(memory_space=pltpu.SMEM)


def kernel(body, out_shape, in_specs, scratch_shapes=()):
    return pl.pallas_call(
        body,
        out_shape=out_shape,
        in_specs=in_specs,
        out_specs=jax.tree.map(lambda _: in_vmem(), out_shape),
        scratch_shapes=list(scratch_shapes),
        compiler_params=pltpu.CompilerParams(vmem_limit_bytes=KERNEL_VMEM),
    )


def normed_of(state, gain):
    scale = lax.rsqrt(jnp.mean(state * state, axis=-1, keepdims=True) + epsilon)
    return (state * scale * gain).astype(narrow)


def pack_body(value_ref, gate_ref, out_ref, pair_ref, part_ref):
    pair_ref[0] = value_ref[...]
    pair_ref[1] = gate_ref[...]
    part_ref[...] = out_ref[...]


def packed(layer, value_proj, gate_proj, out_proj):
    arrays = (value_proj, gate_proj, out_proj)
    return pl.pallas_call(
        pack_body,
        grid=(1,),
        out_shape=(
            jax.ShapeDtypeStruct((2,) + value_proj.shape[1:], narrow),
            jax.ShapeDtypeStruct(out_proj.shape[1:], narrow),
        ),
        in_specs=[
            pl.BlockSpec((None,) + a.shape[1:], lambda i, layer=layer: (layer, 0, 0))
            for a in arrays
        ],
        out_specs=(
            pl.BlockSpec((2,) + value_proj.shape[1:], lambda i: (0, 0, 0)),
            pl.BlockSpec(out_proj.shape[1:], lambda i: (0, 0)),
        ),
        compiler_params=pltpu.CompilerParams(vmem_limit_bytes=KERNEL_VMEM),
    )(*arrays)


def norm_body(prev_ref, tokens_ref, gain_ref, normed_ref):
    halo = prev_ref.shape[0]
    gain = gain_ref[0:1, :]
    normed_ref[:halo, :] = normed_of(prev_ref[...].astype(wide), gain)
    normed_ref[halo:, :] = normed_of(tokens_ref[...].astype(wide), gain)


def gated_conv_body(layer, tap_count, tail, table_ref, normed_ref, dist_ref, taps_ref, *refs):
    *pair_refs, centred_ref, stats_ref, acc_ref, shifted_ref, conv_ref = refs
    width = taps_ref.shape[2]
    halves = width // LANES
    rows = normed_ref.shape[0]
    out_rows = centred_ref.shape[0]
    dist_from = dist_ref.shape[0] - out_rows
    depth = pair_refs[0].shape[1]
    for k, pair in enumerate(pair_refs):
        first = 0 if len(pair_refs) == 1 else pl.multiple_of(table_ref[k] * depth, LANES)
        rows_in = normed_ref[:, pl.ds(first, depth)]
        for part in range(2):
            product = jnp.dot(rows_in, pair[part], preferred_element_type=wide)
            if k == 0:
                acc_ref[part] = product
            else:
                acc_ref[part] += product
    for half in range(halves):
        cols = slice(half * LANES, (half + 1) * LANES)
        value = acc_ref[0, :, cols].astype(narrow).astype(wide)
        gate = acc_ref[1, :, cols].astype(narrow).astype(wide)
        gated = (value * jax.nn.sigmoid(gate)).astype(narrow).astype(wide)
        shifted_ref[half, 0, :, :] = gated
    for half in range(halves):
        for shift in range(1, SUBLANES):
            shifted_ref[half, shift, SUBLANES:, :] = shifted_ref[
                half, 0, SUBLANES - shift : rows - shift, :
            ]

    def block(index, carry):
        base = pl.multiple_of(index * CONV_ROWS, CONV_ROWS)
        dist = dist_ref[pl.ds(pl.multiple_of(base + dist_from, CONV_ROWS), CONV_ROWS), :]
        sums = [jnp.zeros((CONV_ROWS, LANES), wide) for _ in range(halves)]
        for tap in range(tap_count):
            inside = dist >= tap
            start = pl.multiple_of(base + (tail - tap // SUBLANES * SUBLANES), SUBLANES)
            for half in range(halves):
                rows_at = shifted_ref[half, tap % SUBLANES, pl.ds(start, CONV_ROWS), :]
                weight = taps_ref[layer, tap : tap + 1, half * LANES : (half + 1) * LANES]
                sums[half] = sums[half] + jnp.where(inside, weight * rows_at, 0.0)
        for half in range(halves):
            conv_ref[half, pl.ds(base, CONV_ROWS), :] = sums[half]
        return carry

    lax.fori_loop(0, out_rows // CONV_ROWS, block, 0)
    total = conv_ref[0]
    for half in range(1, halves):
        total = total + conv_ref[half]
    mean = jnp.sum(total, axis=1, keepdims=True) / width
    square = jnp.zeros((out_rows, LANES), wide)
    for half in range(halves):
        centred = conv_ref[half] - mean
        centred_ref[:, half * LANES : (half + 1) * LANES] = centred.astype(narrow)
        square = square + centred * centred
    square = jnp.sum(square, axis=1, keepdims=True)
    lane = lax.broadcasted_iota(jnp.int32, (out_rows, LANES), 1)
    both = jnp.where(lane == 0, mean, square)
    padded_rows = stats_ref.shape[1]
    if padded_rows != out_rows:
        both = jnp.concatenate([both, jnp.zeros((padded_rows - out_rows, LANES), wide)])
    stats_ref[...] = both.T[:2, :]


def project_body(layer, far, slots, blocks_at, table_ref, stats_ref, gain_ref, shift_ref, *refs):
    far_norm_refs, refs = refs[: far - 1], refs[far - 1 :]
    centred_refs, refs = refs[:far], refs[far:]
    *piece_refs, share_ref, act_ref = refs
    out_rows, width = centred_refs[0].shape
    tp_count = stats_ref.shape[0]
    stats = jnp.concatenate([stats_ref[j] for j in range(tp_count)])
    stats = stats.T[:out_rows, :]
    means = [stats[:, 2 * j : 2 * j + 1] for j in range(tp_count)]
    mean = functools.reduce(jnp.add, means) / tp_count
    square = sum(
        stats[:, 2 * j + 1 : 2 * j + 2] + width * (means[j] - mean) ** 2 for j in range(tp_count)
    )
    scale = lax.rsqrt(square / (width * tp_count) + epsilon)
    for f, centred in enumerate(centred_refs):
        block = table_ref[blocks_at + f]
        own = jnp.zeros_like(mean)
        for j in range(tp_count):
            own = jnp.where(block == j, means[j], own)
        if f == 0:
            gain, shift = gain_ref[layer : layer + 1, :], shift_ref[layer : layer + 1, :]
        else:
            norms = far_norm_refs[f - 1]
            gain, shift = norms[0, layer : layer + 1, :], norms[1, layer : layer + 1, :]
        normal = gain * (centred[...].astype(wide) + (own - mean)) * scale + shift
        act_ref[f] = (normal * jax.nn.sigmoid(normal)).astype(narrow)
    steps = len(slots) // far
    for k in range(steps):
        share = None
        for f in range(far):
            piece, slot = piece_refs[k * far + f], slots[k * far + f]
            matrix = piece[...] if slot is None else piece[slot]
            product = jnp.dot(act_ref[f], matrix, preferred_element_type=wide)
            share = product if share is None else share + product
        cols = share.shape[1]
        first = 0 if steps == 1 else pl.multiple_of(table_ref[k] * cols, LANES)
        share_ref[:, pl.ds(first, cols)] = share.astype(narrow)


def add_body(layer, tail, is_last, state_count, *refs):
    state_refs, refs = refs[:state_count], refs[state_count:]
    if is_last:
        *share_refs, hidden_ref = refs
    else:
        gain_ref, *share_refs, hidden_ref, normed_ref = refs
    skip, at = tail, 0
    for state_ref in state_refs:
        rows = state_ref.shape[0]
        from_row = min(skip, rows)
        skip = skip - from_row
        count = rows - from_row
        if count == 0:
            continue
        branch = share_refs[0][at : at + count, :].astype(wide)
        for share in share_refs[1:]:
            branch = branch + share[at : at + count, :].astype(wide)
        hidden = (
            state_ref[from_row:, :].astype(wide) + branch.astype(narrow).astype(wide)
        ).astype(narrow)
        hidden_ref[at : at + count, :] = hidden
        if not is_last:
            gain = gain_ref[layer + 1 : layer + 2, :]
            normed_ref[at : at + count, :] = normed_of(hidden.astype(wide), gain)
        at = at + count


def ring_tables(count):
    order = list(range(0, count, 2)) + list(range(count - 1, 0, -2))
    forward = [(order[k], order[(k + 1) % count]) for k in range(count)]
    backward = [(target, source) for source, target in forward]
    steps = [0]
    for k in range(1, count // 2 + 1):
        steps.append(-k)
        if len(steps) < count:
            steps.append(k)
    position = {device: k for k, device in enumerate(order)}
    table = [[order[(position[s] + step) % count] for step in steps] for s in range(count)]
    return forward, backward, table


def ring_gathered(value):
    count = lax.axis_size("sp")
    forward, backward, _ = ring_tables(count)
    chunks = []
    ahead = behind = value
    for _ in range(1, count // 2 + 1):
        ahead = lax.ppermute(ahead, "sp", forward)
        chunks.append(ahead)
        if len(chunks) < count - 1:
            behind = lax.ppermute(behind, "sp", backward)
            chunks.append(behind)
    return chunks


def swap_pairs(count, group, step):
    pairs = []
    for source in range(count):
        lead, at = source // (group * step), source // step % group
        pairs.append((source, (lead * group + (at + 1) % group) * step + source % step))
    return pairs


def ringed(sp_count, *widths):
    return sp_count <= RING_MOST and sp_count % 2 == 0 and not any(w % LANES for w in widths)


def tp_groups(tp_count):
    near = 2 if tp_count % 2 == 0 else 1
    return near, tp_count // near


def on_device(
    tokens, doc_ids, pre_gain, value_proj, gate_proj, out_proj, conv_taps, norm_gain, norm_shift
):
    layer_count = value_proj.shape[0]
    tap_count = conv_taps.shape[1]
    row_count, model_width = tokens.shape
    width = conv_taps.shape[2]
    sp_count, tp_count = lax.axis_size("sp"), lax.axis_size("tp")
    near, far = tp_groups(tp_count)
    far_pairs, near_pairs = swap_pairs(tp_count, far, near), swap_pairs(tp_count, near, 1)
    tail = round_up(tap_count - 1, max(HALO_ALIGN, CONV_ROWS))
    halo = tail * layer_count
    in_ring = ringed(sp_count, value_proj.shape[1], out_proj.shape[2])

    def far_values(value):
        values = [value]
        for _ in range(1, far):
            values.append(lax.ppermute(values[-1], "tp", far_pairs))
        return values

    pair_chunks, out_pieces, out_slots = [], [], []
    own_out = far_values(out_proj) if in_ring else None
    for n in range(layer_count):
        pair, part = packed(n, value_proj, gate_proj, out_proj)
        if in_ring:
            pair_chunks.append([pair] + ring_gathered(pair))
            pieces, slots = list(own_out), [n] * far
            for chunk in ring_gathered(part):
                pieces.extend(far_values(chunk))
                slots.extend([None] * far)
        else:
            pair_chunks.append([lax.all_gather(pair, "sp", axis=1, tiled=True)])
            pieces = [lax.all_gather(value, "sp", axis=1, tiled=True) for value in far_values(part)]
            slots = [None] * far
        out_pieces.append(pieces)
        out_slots.append(slots)

    onward = [(source, source + 1) for source in range(sp_count - 1)]
    prev_docs = lax.ppermute(doc_ids[row_count - halo :] + 1, "sp", onward) - 1
    prev_rows = lax.ppermute(tokens[row_count - halo :], "sp", onward)
    far_norm = far_values(jnp.stack([norm_gain, norm_shift]))[1:]
    docs = jnp.concatenate([prev_docs, doc_ids])
    dist = jnp.zeros((row_count + halo - tail,), jnp.int32)
    for offset in range(1, tap_count):
        first = tail - offset
        dist = dist + (docs[first : first + dist.shape[0]] == docs[tail:]).astype(jnp.int32)
    dist = jnp.broadcast_to(dist[:, None], (dist.shape[0], LANES))

    tp_blocks = []
    for j in range(tp_count):
        lead, at = j // (near * far), j // near % far
        tp_blocks.append([(lead * far + (at - f) % far) * near + j % near for f in range(far)])
    sp_blocks = ring_tables(sp_count)[2] if in_ring else [[0]] * sp_count
    blocks_at = len(sp_blocks[0])
    table = jnp.asarray(
        [[sp_blocks[s] + tp_blocks[j] for j in range(tp_count)] for s in range(sp_count)],
        jnp.int32,
    ).reshape(sp_count * tp_count, -1)
    table = lax.dynamic_index_in_dim(table, lax.axis_index(("sp", "tp")), keepdims=False)

    states = (prev_rows, tokens)
    normed = kernel(
        norm_body, jax.ShapeDtypeStruct((halo + row_count, model_width), narrow), [in_vmem()] * 3
    )(prev_rows, tokens, pre_gain)

    for n in range(layer_count):
        rows = normed.shape[0]
        out_rows = rows - tail
        pairs = pair_chunks[n]
        centred, stats = kernel(
            functools.partial(gated_conv_body, n, tap_count, tail),
            (
                jax.ShapeDtypeStruct((out_rows, width), narrow),
                jax.ShapeDtypeStruct((2, round_up(out_rows, LANES)), wide),
            ),
            [in_smem()] + [in_vmem()] * (3 + len(pairs)),
            [
                pltpu.VMEM((2, rows, width), wide),
                pltpu.VMEM((width // LANES, SUBLANES, rows, LANES), wide),
                pltpu.VMEM((width // LANES, out_rows, LANES), wide),
            ],
        )(table, normed, dist, conv_taps, *pairs)
        far_centred = far_values(centred)
        all_stats = lax.all_gather(stats, "tp")
        pieces = out_pieces[n]
        share = kernel(
            functools.partial(project_body, n, far, out_slots[n], blocks_at),
            jax.ShapeDtypeStruct((out_rows, model_width), narrow),
            [in_smem()] + [in_vmem()] * (3 + far - 1 + far + len(pieces)),
            [pltpu.VMEM((far, out_rows, width), narrow)],
        )(table, all_stats, norm_gain, norm_shift, *far_norm, *far_centred, *pieces)
        shares = [share]
        for _ in range(1, near):
            shares.append(lax.ppermute(shares[-1], "tp", near_pairs))
        is_last = n == layer_count - 1
        shape = jax.ShapeDtypeStruct((out_rows, model_width), narrow)
        gains = () if is_last else (pre_gain,)
        result = kernel(
            functools.partial(add_body, n, tail, is_last, len(states)),
            shape if is_last else (shape, shape),
            [in_vmem()] * (len(states) + len(gains) + len(shares)),
        )(*states, *gains, *shares)
        if is_last:
            return result
        hidden, normed = result
        states = (hidden,)


def solution(mesh):
    return jax.shard_map(
        on_device,
        mesh=mesh,
        in_specs=(
            P("sp", None),
            P("sp"),
            P(),
            P(None, "sp", "tp"),
            P(None, "sp", "tp"),
            P(None, "tp", "sp"),
            P(None, None, "tp"),
            P(None, "tp"),
            P(None, "tp"),
        ),
        out_specs=P("sp", None),
        check_vma=False,
    )
```

```python
import functools

import jax
import jax.numpy as jnp
from jax import lax
from jax.experimental import pallas as pl
from jax.experimental.pallas import tpu as pltpu
from jax.sharding import PartitionSpec as P


epsilon = 1e-06
LANES = 128
SUBLANES = 8
HALO_ALIGN = 16
CONV_ROWS = 32
RING_MOST = 8
KERNEL_VMEM = 20 * 2**20


wide = jnp.float32
narrow = jnp.bfloat16


def round_up(value, step):
    return -(-value // step) * step


def in_vmem():
    return pl.BlockSpec(memory_space=pltpu.VMEM)


def in_smem():
    return pl.BlockSpec(memory_space=pltpu.SMEM)


def kernel(body, out_shape, in_specs, scratch_shapes=()):
    return pl.pallas_call(
        body,
        out_shape=out_shape,
        in_specs=in_specs,
        out_specs=jax.tree.map(lambda _: in_vmem(), out_shape),
        scratch_shapes=list(scratch_shapes),
        compiler_params=pltpu.CompilerParams(vmem_limit_bytes=KERNEL_VMEM),
    )


def normed_of(state, gain):
    scale = lax.rsqrt(jnp.mean(state * state, axis=-1, keepdims=True) + epsilon)
    return (state * scale * gain).astype(narrow)


def copied(sources, targets, sems):
    copies = [
        pltpu.make_async_copy(source, target, sems.at[i])
        for i, (source, target) in enumerate(zip(sources, targets))
    ]
    for copy in copies:
        copy.start()
    for copy in copies:
        copy.wait()


def pack_body(layer, halo, value_ref, gate_ref, *refs):
    if halo == 0:
        pair_ref, sems = refs
        copied([value_ref.at[layer], gate_ref.at[layer]], [pair_ref.at[0], pair_ref.at[1]], sems)
        return
    tokens_ref, gain_ref, shift_ref, pair_ref, tail_ref, norms_ref, sems = refs
    rows = tokens_ref.shape[0]
    copied(
        [
            value_ref.at[layer],
            gate_ref.at[layer],
            tokens_ref.at[pl.ds(rows - halo, halo)],
            gain_ref,
            shift_ref,
        ],
        [pair_ref.at[0], pair_ref.at[1], tail_ref, norms_ref.at[0], norms_ref.at[1]],
        sems,
    )


def packed(layer, value_proj, gate_proj, halo=0, extra=()):
    shapes = [jax.ShapeDtypeStruct((2,) + value_proj.shape[1:], narrow)]
    if halo:
        tokens, gain, _ = extra
        shapes.append(jax.ShapeDtypeStruct((halo, tokens.shape[1]), narrow))
        shapes.append(jax.ShapeDtypeStruct((2,) + gain.shape, wide))
    return pl.pallas_call(
        functools.partial(pack_body, layer, halo),
        out_shape=tuple(shapes),
        in_specs=[pl.BlockSpec(memory_space=pl.ANY)] * (2 + len(extra)),
        out_specs=tuple(in_vmem() for _ in shapes),
        scratch_shapes=[pltpu.SemaphoreType.DMA((5 if halo else 2,))],
        compiler_params=pltpu.CompilerParams(vmem_limit_bytes=KERNEL_VMEM),
    )(value_proj, gate_proj, *extra)


def norm_body(prev_ref, tokens_ref, gain_ref, normed_ref):
    halo = prev_ref.shape[0]
    gain = gain_ref[0:1, :]
    normed_ref[:halo, :] = normed_of(prev_ref[...].astype(wide), gain)
    normed_ref[halo:, :] = normed_of(tokens_ref[...].astype(wide), gain)


def gated_conv_body(
    layer, tap_count, tail, split, table_ref, normed_ref, dist_ref, taps_ref, *refs
):
    *pair_refs, centred_ref, stats_ref, acc_ref, shifted_ref, conv_ref = refs
    pairs = [(pair.at[0], pair.at[1]) for pair in (pair_refs[:-2] if split else pair_refs)]
    if split:
        pairs.append(tuple(pair_refs[-2:]))
    width = taps_ref.shape[2]
    halves = width // LANES
    rows = normed_ref.shape[0]
    out_rows = centred_ref.shape[0]
    dist_from = dist_ref.shape[0] - out_rows
    depth = pair_refs[0].shape[1]
    for k, pair in enumerate(pairs):
        first = 0 if len(pairs) == 1 else pl.multiple_of(table_ref[k] * depth, LANES)
        rows_in = normed_ref[:, pl.ds(first, depth)]
        for part in range(2):
            product = jnp.dot(rows_in, pair[part][...], preferred_element_type=wide)
            if k == 0:
                acc_ref[part] = product
            else:
                acc_ref[part] += product
    for half in range(halves):
        cols = slice(half * LANES, (half + 1) * LANES)
        value = acc_ref[0, :, cols].astype(narrow).astype(wide)
        gate = acc_ref[1, :, cols].astype(narrow).astype(wide)
        gated = (value * jax.nn.sigmoid(gate)).astype(narrow).astype(wide)
        shifted_ref[half, 0, :, :] = gated
    for half in range(halves):
        for shift in range(1, SUBLANES):
            shifted_ref[half, shift, SUBLANES:, :] = shifted_ref[
                half, 0, SUBLANES - shift : rows - shift, :
            ]

    def block(index, carry):
        base = pl.multiple_of(index * CONV_ROWS, CONV_ROWS)
        dist = dist_ref[pl.ds(pl.multiple_of(base + dist_from, CONV_ROWS), CONV_ROWS), :]
        sums = [jnp.zeros((CONV_ROWS, LANES), wide) for _ in range(halves)]
        for tap in range(tap_count):
            inside = dist >= tap
            start = pl.multiple_of(base + (tail - tap // SUBLANES * SUBLANES), SUBLANES)
            for half in range(halves):
                rows_at = shifted_ref[half, tap % SUBLANES, pl.ds(start, CONV_ROWS), :]
                weight = taps_ref[layer, tap : tap + 1, half * LANES : (half + 1) * LANES]
                sums[half] = sums[half] + jnp.where(inside, weight * rows_at, 0.0)
        for half in range(halves):
            conv_ref[half, pl.ds(base, CONV_ROWS), :] = sums[half]
        return carry

    lax.fori_loop(0, out_rows // CONV_ROWS, block, 0)
    total = conv_ref[0]
    for half in range(1, halves):
        total = total + conv_ref[half]
    mean = jnp.sum(total, axis=1, keepdims=True) / width
    square = jnp.zeros((out_rows, LANES), wide)
    for half in range(halves):
        centred = conv_ref[half] - mean
        centred_ref[:, half * LANES : (half + 1) * LANES] = centred.astype(narrow)
        square = square + centred * centred
    square = jnp.sum(square, axis=1, keepdims=True)
    lane = lax.broadcasted_iota(jnp.int32, (out_rows, LANES), 1)
    both = jnp.where(lane == 0, mean, square)
    padded_rows = stats_ref.shape[1]
    if padded_rows != out_rows:
        both = jnp.concatenate([both, jnp.zeros((padded_rows - out_rows, LANES), wide)])
    stats_ref[...] = both.T[:2, :]


def summed(values):
    return functools.reduce(jnp.add, values)


def project_body(layer, near, far, slots, table_ref, gain_ref, shift_ref, *refs):
    far_norm_refs, refs = refs[: far - 1], refs[far - 1 :]
    stats_refs, refs = refs[: far * near], refs[far * near :]
    centred_refs, refs = refs[:far], refs[far:]
    *piece_refs, share_ref, act_ref = refs
    out_rows, width = centred_refs[0].shape
    count = far * near
    fill = jnp.zeros((round_up(2 * count, SUBLANES) - 2 * count, stats_refs[0].shape[1]), wide)
    stats = jnp.concatenate([ref[...] for ref in stats_refs] + ([fill] if fill.size else []))
    stats = stats.T[:out_rows, :]
    means = [stats[:, 2 * j : 2 * j + 1] for j in range(count)]
    squares = [stats[:, 2 * j + 1 : 2 * j + 2] for j in range(count)]
    mean = summed([summed(means[f * near : (f + 1) * near]) for f in range(far)]) / count
    squares = [square + width * (own - mean) ** 2 for square, own in zip(squares, means)]
    square = summed([summed(squares[f * near : (f + 1) * near]) for f in range(far)])
    scale = lax.rsqrt(square / (width * count) + epsilon)
    for f, centred in enumerate(centred_refs):
        own = means[f * near]
        if f == 0:
            gain, shift = gain_ref[layer : layer + 1, :], shift_ref[layer : layer + 1, :]
        else:
            norms = far_norm_refs[f - 1]
            gain, shift = norms[0, layer : layer + 1, :], norms[1, layer : layer + 1, :]
        normal = gain * (centred[...].astype(wide) + (own - mean)) * scale + shift
        act_ref[f] = (normal * jax.nn.sigmoid(normal)).astype(narrow)
    steps = len(slots) // far
    for k in range(steps):
        share = None
        for f in range(far):
            piece, slot = piece_refs[k * far + f], slots[k * far + f]
            matrix = piece[...] if slot is None else piece[slot]
            product = jnp.dot(act_ref[f], matrix, preferred_element_type=wide)
            share = product if share is None else share + product
        cols = share.shape[1]
        first = 0 if steps == 1 else pl.multiple_of(table_ref[k] * cols, LANES)
        share_ref[:, pl.ds(first, cols)] = share.astype(narrow)


def add_body(layer, tail, is_last, state_count, *refs):
    state_refs, refs = refs[:state_count], refs[state_count:]
    if is_last:
        *share_refs, hidden_ref = refs
    else:
        gain_ref, *share_refs, hidden_ref, normed_ref = refs
    skip, at = tail, 0
    for state_ref in state_refs:
        rows = state_ref.shape[0]
        from_row = min(skip, rows)
        skip = skip - from_row
        count = rows - from_row
        if count == 0:
            continue
        branch = share_refs[0][at : at + count, :].astype(wide)
        for share in share_refs[1:]:
            branch = branch + share[at : at + count, :].astype(wide)
        hidden = (
            state_ref[from_row:, :].astype(wide) + branch.astype(narrow).astype(wide)
        ).astype(narrow)
        hidden_ref[at : at + count, :] = hidden
        if not is_last:
            gain = gain_ref[layer + 1 : layer + 2, :]
            normed_ref[at : at + count, :] = normed_of(hidden.astype(wide), gain)
        at = at + count


def ring_tables(count):
    order = list(range(0, count, 2)) + list(range(count - 1, 0, -2))
    forward = [(order[k], order[(k + 1) % count]) for k in range(count)]
    backward = [(target, source) for source, target in forward]
    steps = [0]
    for k in range(1, count // 2 + 1):
        steps.append(-k)
        if len(steps) < count:
            steps.append(k)
    position = {device: k for k, device in enumerate(order)}
    table = [[order[(position[s] + step) % count] for step in steps] for s in range(count)]
    return forward, backward, table


def ring_gathered(value):
    count = lax.axis_size("sp")
    forward, backward, _ = ring_tables(count)
    chunks = []
    ahead = behind = value
    for k in range(1, count // 2 + 1):
        if 2 * k == count:
            ahead, behind = ahead[0], behind[1]
        ahead = lax.ppermute(ahead, "sp", forward)
        behind = lax.ppermute(behind, "sp", backward)
        chunks.extend((ahead, behind))
    return chunks


def group_pairs(count, near, far, near_step, far_step):
    pairs = []
    for source in range(count):
        at_far, at_near = source // near, source % near
        target = (at_far + far_step) % far * near + (at_near + near_step) % near
        pairs.append((source, target))
    return pairs


def ringed(sp_count, *widths):
    return sp_count <= RING_MOST and sp_count % 2 == 0 and not any(w % LANES for w in widths)


def tp_groups(tp_count):
    near = 2 if tp_count % 2 == 0 else 1
    return near, tp_count // near


def on_device(
    tokens, doc_ids, pre_gain, value_proj, gate_proj, out_proj, conv_taps, norm_gain, norm_shift
):
    layer_count = value_proj.shape[0]
    tap_count = conv_taps.shape[1]
    row_count, model_width = tokens.shape
    width = conv_taps.shape[2]
    sp_count, tp_count = lax.axis_size("sp"), lax.axis_size("tp")
    near, far = tp_groups(tp_count)
    far_pairs = group_pairs(tp_count, near, far, 0, 1)
    near_pairs = group_pairs(tp_count, near, far, 1, 0)
    tail = round_up(tap_count - 1, max(HALO_ALIGN, CONV_ROWS))
    halo = tail * layer_count
    in_ring = layer_count == 2 and ringed(sp_count, value_proj.shape[1], out_proj.shape[2])

    def far_values(value):
        values = [value]
        for _ in range(1, far):
            values.append(lax.ppermute(values[-1], "tp", far_pairs))
        return values

    packs = [packed(n, value_proj, gate_proj) for n in range(layer_count - 1)]
    packs.append(
        packed(layer_count - 1, value_proj, gate_proj, halo, (tokens, norm_gain, norm_shift))
    )
    _, tail_rows, norms = packs[-1]
    pair_chunks, out_pieces, out_slots = [], [], []
    if in_ring:
        chunks = [out_proj] + ring_gathered(out_proj)
        chunks = [far_values(chunk) for chunk in chunks]
    for n in range(layer_count):
        pair = packs[n][0]
        if in_ring:
            pair_chunks.append([pair] + ring_gathered(pair))
            pieces = [piece for k in range(len(chunks) - 2) for piece in chunks[k]]
            slots = [n] * len(pieces) + [None] * far
            pieces.extend(chunks[len(chunks) - 2 + n])
        else:
            pair_chunks.append([lax.all_gather(pair, "sp", axis=1, tiled=True)])
            pieces = [
                lax.all_gather(value, "sp", axis=1, tiled=True)
                for value in far_values(out_proj[n])
            ]
            slots = [None] * far
        out_pieces.append(pieces)
        out_slots.append(slots)

    onward = [(source, source + 1) for source in range(sp_count - 1)]
    prev_docs = lax.ppermute(doc_ids[row_count - halo :] + 1, "sp", onward) - 1
    prev_rows = lax.ppermute(tail_rows, "sp", onward)
    far_norm = far_values(norms)[1:]
    docs = jnp.concatenate([prev_docs, doc_ids])
    dist = jnp.zeros((row_count + halo - tail,), jnp.int32)
    for offset in range(1, tap_count):
        first = tail - offset
        dist = dist + (docs[first : first + dist.shape[0]] == docs[tail:]).astype(jnp.int32)
    dist = jnp.broadcast_to(dist[:, None], (dist.shape[0], LANES))

    sp_blocks = ring_tables(sp_count)[2] if in_ring else [[0]] * sp_count
    table = jnp.asarray(sp_blocks, jnp.int32)
    table = lax.dynamic_index_in_dim(table, lax.axis_index("sp"), keepdims=False)

    states = (prev_rows, tokens)
    normed = kernel(
        norm_body, jax.ShapeDtypeStruct((halo + row_count, model_width), narrow), [in_vmem()] * 3
    )(prev_rows, tokens, pre_gain)

    for n in range(layer_count):
        rows = normed.shape[0]
        out_rows = rows - tail
        pairs = pair_chunks[n]
        centred, stats = kernel(
            functools.partial(gated_conv_body, n, tap_count, tail, in_ring),
            (
                jax.ShapeDtypeStruct((out_rows, width), narrow),
                jax.ShapeDtypeStruct((2, round_up(out_rows, LANES)), wide),
            ),
            [in_smem()] + [in_vmem()] * (3 + len(pairs)),
            [
                pltpu.VMEM((2, rows, width), wide),
                pltpu.VMEM((width // LANES, SUBLANES, rows, LANES), wide),
                pltpu.VMEM((width // LANES, out_rows, LANES), wide),
            ],
        )(table, normed, dist, conv_taps, *pairs)
        far_centred = far_values(centred)
        all_stats = [stats]
        for place in range(1, tp_count):
            steps = group_pairs(tp_count, near, far, place % near, place // near)
            all_stats.append(lax.ppermute(stats, "tp", steps))
        pieces = out_pieces[n]
        share = kernel(
            functools.partial(project_body, n, near, far, out_slots[n]),
            jax.ShapeDtypeStruct((out_rows, model_width), narrow),
            [in_smem()] + [in_vmem()] * (2 + far - 1 + tp_count + far + len(pieces)),
            [pltpu.VMEM((far, out_rows, width), narrow)],
        )(table, norm_gain, norm_shift, *far_norm, *all_stats, *far_centred, *pieces)
        shares = [share]
        for _ in range(1, near):
            shares.append(lax.ppermute(shares[-1], "tp", near_pairs))
        is_last = n == layer_count - 1
        shape = jax.ShapeDtypeStruct((out_rows, model_width), narrow)
        gains = () if is_last else (pre_gain,)
        result = kernel(
            functools.partial(add_body, n, tail, is_last, len(states)),
            shape if is_last else (shape, shape),
            [in_vmem()] * (len(states) + len(gains) + len(shares)),
        )(*states, *gains, *shares)
        if is_last:
            return result
        hidden, normed = result
        states = (hidden,)


def solution(mesh):
    return jax.shard_map(
        on_device,
        mesh=mesh,
        in_specs=(
            P("sp", None),
            P("sp"),
            P(),
            P(None, "sp", "tp"),
            P(None, "sp", "tp"),
            P(None, "tp", "sp"),
            P(None, None, "tp"),
            P(None, "tp"),
            P(None, "tp"),
        ),
        out_specs=P("sp", None),
        check_vma=False,
    )
```

```python
import functools

import jax
import jax.numpy as jnp
from jax import lax
from jax.experimental import pallas as pl
from jax.experimental.pallas import tpu as pltpu
from jax.sharding import PartitionSpec as P


epsilon = 1e-06
LANES = 128
SUBLANES = 8
HALO_ALIGN = 16
CONV_ROWS = 32
RING_MOST = 8
KERNEL_VMEM = 20 * 2**20
PACK_FLOPS = 2 * 10**9
PACK_BYTES = 8 * 10**6


wide = jnp.float32
narrow = jnp.bfloat16


def round_up(value, step):
    return -(-value // step) * step


def in_vmem():
    return pl.BlockSpec(memory_space=pltpu.VMEM)


def in_hbm():
    return pl.BlockSpec(memory_space=pl.ANY)


def kernel(body, out_shape, in_specs, scratch_shapes=()):
    return pl.pallas_call(
        body,
        out_shape=out_shape,
        in_specs=in_specs,
        out_specs=jax.tree.map(lambda _: in_vmem(), out_shape),
        scratch_shapes=list(scratch_shapes),
        compiler_params=pltpu.CompilerParams(vmem_limit_bytes=KERNEL_VMEM),
    )


def normed_of(state, gain):
    scale = lax.rsqrt(jnp.mean(state * state, axis=-1, keepdims=True) + epsilon)
    return (state * scale * gain).astype(narrow)


def copied(sources, targets, sems):
    copies = [
        pltpu.make_async_copy(source, target, sems.at[i])
        for i, (source, target) in enumerate(zip(sources, targets))
    ]
    for copy in copies:
        copy.start()
    for copy in copies:
        copy.wait()


def pack_body(layer, halo, near, value_ref, gate_ref, *refs):
    if halo == 0:
        pair_ref, sems = refs
        copied([value_ref.at[layer], gate_ref.at[layer]], [pair_ref.at[0], pair_ref.at[1]], sems)
        return
    docs_ref, tokens_ref, pair_ref, tail_ref, sems = refs
    rows, model_width = tokens_ref.shape
    span = round_up(halo, LANES)
    docs = docs_ref[...].reshape(1, rows)[:, rows - span :] + 1
    row = lax.broadcasted_iota(jnp.int32, (LANES, span), 0)
    docs = jnp.where(row == 0, docs // 256, jnp.where(row == 1, docs % 256, 0))
    docs = docs.astype(wide).T[span - halo :, :].astype(narrow)
    part = halo // near
    place = lax.axis_index("tp") % near
    for other in range(near):

        @pl.when(place == other)
        def _(other=other):
            tail_ref[:, model_width:] = docs[other * part : (other + 1) * part, :]

    copied(
        [
            value_ref.at[layer],
            gate_ref.at[layer],
            tokens_ref.at[pl.ds(pl.multiple_of(rows - halo + place * part, HALO_ALIGN), part)],
        ],
        [pair_ref.at[0], pair_ref.at[1], tail_ref.at[:, pl.ds(0, model_width)]],
        sems,
    )


def packed(layer, value_proj, gate_proj, halo=0, near=1, extra=()):
    shapes = [jax.ShapeDtypeStruct((2,) + value_proj.shape[1:], narrow)]
    if halo:
        _, tokens = extra
        shapes.append(jax.ShapeDtypeStruct((halo // near, tokens.shape[1] + LANES), narrow))
    return pl.pallas_call(
        functools.partial(pack_body, layer, halo, near),
        out_shape=tuple(shapes),
        in_specs=[in_hbm()] * 2 + [in_vmem()] * min(1, len(extra)) + [in_hbm()] * (len(extra) - 1),
        out_specs=tuple(in_vmem() for _ in shapes),
        scratch_shapes=[pltpu.SemaphoreType.DMA((3 if halo else 2,))],
        cost_estimate=pl.CostEstimate(flops=PACK_FLOPS, bytes_accessed=PACK_BYTES, transcendentals=0),
        compiler_params=pltpu.CompilerParams(vmem_limit_bytes=KERNEL_VMEM),
    )(value_proj, gate_proj, *extra)


def norm_body(tail, near, tokens_ref, docs_ref, gain_ref, *refs):
    prev_refs, (normed_ref, dist_ref, state_ref, run_ref) = refs[:near], refs[near:]
    row_count, model_width = tokens_ref.shape
    halo = normed_ref.shape[0] - row_count
    part = halo // near
    rows = halo + row_count
    lead = run_ref.shape[0] - rows
    gain = gain_ref[0:1, :]
    place = lax.axis_index("tp") % near
    for step, prev_ref in enumerate(prev_refs):
        first = pl.multiple_of((place - step + near) % near * part, HALO_ALIGN)
        prev = prev_ref[:, :model_width]
        state_ref[pl.ds(first, part), :] = prev
        normed_ref[pl.ds(first, part), :] = normed_of(prev.astype(wide), gain)
        docs = prev_ref[:, model_width:].astype(wide)
        docs = jnp.broadcast_to(docs[:, 0:1] * 256 + docs[:, 1:2], (part, LANES))
        run_ref[pl.ds(pl.multiple_of(lead + first, SUBLANES), part), :] = docs
    normed_ref[halo:, :] = normed_of(tokens_ref[...].astype(wide), gain)
    own_docs = docs_ref[...].reshape(1, row_count).astype(wide)
    own_docs = jnp.broadcast_to(own_docs, (SUBLANES, row_count)).T[:, 0:1] + 1
    run_ref[:lead, :] = jnp.full((lead, LANES), -1.0, wide)
    run_ref[lead + halo :, :] = jnp.broadcast_to(own_docs, (row_count, LANES))
    same = run_ref[lead:, :] == run_ref[lead - 1 : lead - 1 + rows, :]
    run = jnp.where(same, 1.0, 0.0)
    run_ref[:lead, :] = jnp.zeros((lead, LANES), wide)
    reach = 1
    while reach < tail:
        run_ref[lead:, :] = run
        run = jnp.where(run == reach, reach + run_ref[lead - reach : lead - reach + rows, :], run)
        reach = 2 * reach
    dist_ref[...] = run[tail:, :]


def chunk_start(places, k, size):
    if places is None:
        return 0
    count, steps = places
    return pl.multiple_of(ring_place(count, steps[k]) * size, LANES)


def gated_conv_body(
    layer, tap_count, tail, places, normed_ref, dist_ref, taps_ref, *refs
):
    *pair_refs, centred_ref, stats_ref, acc_ref, shifted_ref, conv_ref = refs
    pairs = [(pair.at[0], pair.at[1]) for pair in (pair_refs[:-2] if places else pair_refs)]
    if places:
        pairs.append(tuple(pair_refs[-2:]))
    width = taps_ref.shape[2]
    halves = width // LANES
    rows = normed_ref.shape[0]
    out_rows = centred_ref.shape[0]
    dist_from = dist_ref.shape[0] - out_rows
    depth = pair_refs[0].shape[1]
    for k, pair in enumerate(pairs):
        first = chunk_start(places, k, depth)
        rows_in = normed_ref[:, pl.ds(first, depth)]
        for part in range(2):
            product = jnp.dot(rows_in, pair[part][...], preferred_element_type=wide)
            if k == 0:
                acc_ref[part] = product
            else:
                acc_ref[part] += product
    for half in range(halves):
        cols = slice(half * LANES, (half + 1) * LANES)
        value = acc_ref[0, :, cols].astype(narrow).astype(wide)
        gate = acc_ref[1, :, cols].astype(narrow).astype(wide)
        gated = (value * jax.nn.sigmoid(gate)).astype(narrow).astype(wide)
        shifted_ref[half, 0, :, :] = gated
    for half in range(halves):
        for shift in range(1, SUBLANES):
            shifted_ref[half, shift, SUBLANES:, :] = shifted_ref[
                half, 0, SUBLANES - shift : rows - shift, :
            ]

    def block(index, carry):
        base = pl.multiple_of(index * CONV_ROWS, CONV_ROWS)
        dist = dist_ref[pl.ds(pl.multiple_of(base + dist_from, CONV_ROWS), CONV_ROWS), :]
        sums = [jnp.zeros((CONV_ROWS, LANES), wide) for _ in range(halves)]
        for tap in range(tap_count):
            inside = dist >= tap
            start = pl.multiple_of(base + (tail - tap // SUBLANES * SUBLANES), SUBLANES)
            for half in range(halves):
                rows_at = shifted_ref[half, tap % SUBLANES, pl.ds(start, CONV_ROWS), :]
                weight = taps_ref[tap, layer : layer + 1, half * LANES : (half + 1) * LANES]
                sums[half] = sums[half] + jnp.where(inside, weight * rows_at, 0.0)
        for half in range(halves):
            conv_ref[half, pl.ds(base, CONV_ROWS), :] = sums[half]
        return carry

    lax.fori_loop(0, out_rows // CONV_ROWS, block, 0)
    total = conv_ref[0]
    for half in range(1, halves):
        total = total + conv_ref[half]
    mean = jnp.sum(total, axis=1, keepdims=True) / width
    square = jnp.zeros((out_rows, LANES), wide)
    for half in range(halves):
        centred = conv_ref[half] - mean
        centred_ref[:, half * LANES : (half + 1) * LANES] = centred.astype(narrow)
        square = square + centred * centred
    square = jnp.sum(square, axis=1, keepdims=True)
    lane = lax.broadcasted_iota(jnp.int32, (out_rows, LANES), 1)
    both = jnp.where(lane == 0, mean, square)
    padded_rows = stats_ref.shape[1]
    if padded_rows != out_rows:
        both = jnp.concatenate([both, jnp.zeros((padded_rows - out_rows, LANES), wide)])
    stats_ref[...] = both.T[:2, :]


def summed(values):
    return functools.reduce(jnp.add, values)


def project_body(layer, near, far, slots, places, *refs):
    gain_refs, shift_refs, refs = refs[:far], refs[far : 2 * far], refs[2 * far :]
    stats_refs, refs = refs[: far * near], refs[far * near :]
    centred_refs, refs = refs[:far], refs[far:]
    *piece_refs, share_ref, act_ref = refs
    out_rows, width = centred_refs[0].shape
    count = far * near
    fill = jnp.zeros((round_up(2 * count, SUBLANES) - 2 * count, stats_refs[0].shape[1]), wide)
    stats = jnp.concatenate([ref[...] for ref in stats_refs] + ([fill] if fill.size else []))
    stats = stats.T[:out_rows, :]
    means = [stats[:, 2 * j : 2 * j + 1] for j in range(count)]
    squares = [stats[:, 2 * j + 1 : 2 * j + 2] for j in range(count)]
    mean = summed([summed(means[f * near : (f + 1) * near]) for f in range(far)]) / count
    squares = [square + width * (own - mean) ** 2 for square, own in zip(squares, means)]
    square = summed([summed(squares[f * near : (f + 1) * near]) for f in range(far)])
    scale = lax.rsqrt(square / (width * count) + epsilon)
    for f, centred in enumerate(centred_refs):
        own = means[f * near]
        gain, shift = gain_refs[f][layer : layer + 1, :], shift_refs[f][layer : layer + 1, :]
        normal = gain * (centred[...].astype(wide) + (own - mean)) * scale + shift
        act_ref[f] = (normal * jax.nn.sigmoid(normal)).astype(narrow)
    steps = len(slots) // far
    for k in range(steps):
        share = None
        for f in range(far):
            piece, slot = piece_refs[k * far + f], slots[k * far + f]
            matrix = piece[...] if slot is None else piece[slot]
            product = jnp.dot(act_ref[f], matrix, preferred_element_type=wide)
            share = product if share is None else share + product
        cols = share.shape[1]
        first = chunk_start(places, k, cols)
        share_ref[:, pl.ds(first, cols)] = share.astype(narrow)


def add_body(layer, tail, is_last, state_count, *refs):
    state_refs, refs = refs[:state_count], refs[state_count:]
    if is_last:
        *share_refs, hidden_ref = refs
    else:
        gain_ref, *share_refs, hidden_ref, normed_ref = refs
    skip, at = tail, 0
    model_width = hidden_ref.shape[1]
    for state_ref in state_refs:
        rows = state_ref.shape[0]
        from_row = min(skip, rows)
        skip = skip - from_row
        count = rows - from_row
        if count == 0:
            continue
        branch = share_refs[0][at : at + count, :].astype(wide)
        for share in share_refs[1:]:
            branch = branch + share[at : at + count, :].astype(wide)
        hidden = (
            state_ref[from_row:, :model_width].astype(wide) + branch.astype(narrow).astype(wide)
        ).astype(narrow)
        hidden_ref[at : at + count, :] = hidden
        if not is_last:
            gain = gain_ref[layer + 1 : layer + 2, :]
            normed_ref[at : at + count, :] = normed_of(hidden.astype(wide), gain)
        at = at + count


def ring_place(count, step):
    index = lax.axis_index("sp")
    odd = index % 2
    position = jnp.where(odd == 1, count - 1 - index // 2, index // 2)
    position = (position + step + count) % count
    return jnp.where(
        position < count // 2, 2 * position, 2 * (count - 1 - position) + 1
    )


def ring_tables(count):
    order = list(range(0, count, 2)) + list(range(count - 1, 0, -2))
    forward = [(order[k], order[(k + 1) % count]) for k in range(count)]
    backward = [(target, source) for source, target in forward]
    steps = [0]
    for k in range(1, count // 2 + 1):
        steps.append(-k)
        if len(steps) < count:
            steps.append(k)
    return forward, backward, steps


def ring_gathered(value):
    count = lax.axis_size("sp")
    forward, backward, _ = ring_tables(count)
    chunks = []
    ahead = behind = value
    for k in range(1, count // 2 + 1):
        if 2 * k == count:
            ahead, behind = ahead[0], behind[1]
        ahead = lax.ppermute(ahead, "sp", forward)
        behind = lax.ppermute(behind, "sp", backward)
        chunks.extend((ahead, behind))
    return chunks


def group_pairs(count, near, far, near_step, far_step):
    pairs = []
    for source in range(count):
        at_far, at_near = source // near, source % near
        target = (at_far + far_step) % far * near + (at_near + near_step) % near
        pairs.append((source, target))
    return pairs


def ringed(sp_count, *widths):
    return sp_count <= RING_MOST and sp_count % 2 == 0 and not any(w % LANES for w in widths)


def tp_groups(tp_count):
    near = 2 if tp_count % 2 == 0 else 1
    return near, tp_count // near


def on_device(
    tokens, doc_ids, pre_gain, value_proj, gate_proj, out_proj, conv_taps, norm_gain, norm_shift
):
    layer_count = value_proj.shape[0]
    tap_count = conv_taps.shape[1]
    row_count, model_width = tokens.shape
    width = conv_taps.shape[2]
    sp_count, tp_count = lax.axis_size("sp"), lax.axis_size("tp")
    near, far = tp_groups(tp_count)
    far_pairs = group_pairs(tp_count, near, far, 0, 1)
    near_pairs = group_pairs(tp_count, near, far, 1, 0)
    tail = round_up(tap_count - 1, max(HALO_ALIGN, CONV_ROWS))
    halo = tail * layer_count
    in_ring = layer_count == 2 and ringed(sp_count, value_proj.shape[1], out_proj.shape[2])

    def far_values(value):
        values = [value]
        for _ in range(1, far):
            values.append(lax.ppermute(values[-1], "tp", far_pairs))
        return values

    docs = doc_ids
    packs = [packed(n, value_proj, gate_proj) for n in range(layer_count - 1)]
    packs.append(packed(layer_count - 1, value_proj, gate_proj, halo, near, (docs, tokens)))
    tail_part = packs[-1][1]
    pair_chunks, out_pieces, out_slots = [], [], []
    if in_ring:
        chunks = [out_proj] + ring_gathered(out_proj)
        chunks = [far_values(chunk) for chunk in chunks]
    for n in range(layer_count):
        pair = packs[n][0]
        if in_ring:
            pair_chunks.append([pair] + ring_gathered(pair))
            pieces = [piece for k in range(len(chunks) - 2) for piece in chunks[k]]
            slots = [n] * len(pieces) + [None] * far
            pieces.extend(chunks[len(chunks) - 2 + n])
        else:
            pair_chunks.append([lax.all_gather(pair, "sp", axis=1, tiled=True)])
            pieces = [
                lax.all_gather(value, "sp", axis=1, tiled=True)
                for value in far_values(out_proj[n])
            ]
            slots = [None] * far
        out_pieces.append(pieces)
        out_slots.append(slots)

    onward = [(source, source + 1) for source in range(sp_count - 1)]
    prev_parts = [lax.ppermute(tail_part, "sp", onward)]
    for _ in range(1, near):
        prev_parts.append(lax.ppermute(prev_parts[-1], "tp", near_pairs))
    gains, shifts = far_values(norm_gain), far_values(norm_shift)
    places = (sp_count, ring_tables(sp_count)[2]) if in_ring else None

    taps = jnp.transpose(conv_taps, (1, 0, 2))
    normed, dist, prev_state = kernel(
        functools.partial(norm_body, tail, near),
        (
            jax.ShapeDtypeStruct((halo + row_count, model_width), narrow),
            jax.ShapeDtypeStruct((halo + row_count - tail, LANES), wide),
            jax.ShapeDtypeStruct((halo, model_width), narrow),
        ),
        [in_vmem()] * (3 + near),
        [pltpu.VMEM((tail + halo + row_count, LANES), wide)],
    )(tokens, docs, pre_gain, *prev_parts)
    states = (prev_state, tokens)

    for n in range(layer_count):
        rows = normed.shape[0]
        out_rows = rows - tail
        pairs = pair_chunks[n]
        centred, stats = kernel(
            functools.partial(gated_conv_body, n, tap_count, tail, places),
            (
                jax.ShapeDtypeStruct((out_rows, width), narrow),
                jax.ShapeDtypeStruct((2, round_up(out_rows, LANES)), wide),
            ),
            [in_vmem()] * (3 + len(pairs)),
            [
                pltpu.VMEM((2, rows, width), wide),
                pltpu.VMEM((width // LANES, SUBLANES, rows, LANES), wide),
                pltpu.VMEM((width // LANES, out_rows, LANES), wide),
            ],
        )(normed, dist, taps, *pairs)
        far_centred = far_values(centred)
        all_stats = [stats]
        for place in range(1, tp_count):
            steps = group_pairs(tp_count, near, far, place % near, place // near)
            all_stats.append(lax.ppermute(stats, "tp", steps))
        pieces = out_pieces[n]
        share = kernel(
            functools.partial(project_body, n, near, far, out_slots[n], places),
            jax.ShapeDtypeStruct((out_rows, model_width), narrow),
            [in_vmem()] * (3 * far + tp_count + len(pieces)),
            [pltpu.VMEM((far, out_rows, width), narrow)],
        )(*gains, *shifts, *all_stats, *far_centred, *pieces)
        shares = [share]
        for _ in range(1, near):
            shares.append(lax.ppermute(shares[-1], "tp", near_pairs))
        is_last = n == layer_count - 1
        shape = jax.ShapeDtypeStruct((out_rows, model_width), narrow)
        next_gain = () if is_last else (pre_gain,)
        result = kernel(
            functools.partial(add_body, n, tail, is_last, len(states)),
            shape if is_last else (shape, shape),
            [in_vmem()] * (len(states) + len(next_gain) + len(shares)),
        )(*states, *next_gain, *shares)
        if is_last:
            return result
        hidden, normed = result
        states = (hidden,)


def solution(mesh):
    return jax.shard_map(
        on_device,
        mesh=mesh,
        in_specs=(
            P("sp", None),
            P("sp"),
            P(),
            P(None, "sp", "tp"),
            P(None, "sp", "tp"),
            P(None, "tp", "sp"),
            P(None, None, "tp"),
            P(None, "tp"),
            P(None, "tp"),
        ),
        out_specs=P("sp", None),
        check_vma=False,
    )
```

```python
import functools

import jax
import jax.numpy as jnp
from jax import lax
from jax.experimental import pallas as pl
from jax.experimental.pallas import tpu as pltpu
from jax.sharding import PartitionSpec as P


epsilon = 1e-06
LANES = 128
SUBLANES = 8
HALO_ALIGN = 16
CONV_ROWS = 32
RING_MOST = 8
KERNEL_VMEM = 20 * 2**20
PACK_FLOPS = 2 * 10**9
PACK_BYTES = 8 * 10**6
PRODUCTS_AHEAD = (5, 7)
SHARE_PARTS = 2


wide = jnp.float32
narrow = jnp.bfloat16


def round_up(value, step):
    return -(-value // step) * step


def in_vmem():
    return pl.BlockSpec(memory_space=pltpu.VMEM)


def in_smem():
    return pl.BlockSpec(memory_space=pltpu.SMEM)


def in_hbm():
    return pl.BlockSpec(memory_space=pl.ANY)


def kernel(body, out_shape, in_specs, scratch_shapes=()):
    return pl.pallas_call(
        body,
        out_shape=out_shape,
        in_specs=in_specs,
        out_specs=jax.tree.map(
            lambda shape: in_smem() if len(shape.shape) == 1 else in_vmem(), out_shape
        ),
        scratch_shapes=list(scratch_shapes),
        compiler_params=pltpu.CompilerParams(vmem_limit_bytes=KERNEL_VMEM),
    )


def normed_of(state, gain):
    scale = lax.rsqrt(jnp.mean(state * state, axis=-1, keepdims=True) + epsilon)
    return (state * scale * gain).astype(narrow)


def copied(sources, targets, sems):
    copies = [
        pltpu.make_async_copy(source, target, sems.at[i])
        for i, (source, target) in enumerate(zip(sources, targets))
    ]
    for copy in copies:
        copy.start()
    for copy in copies:
        copy.wait()


def pack_body(layer, halo, near, value_ref, gate_ref, *refs):
    if halo == 0:
        pair_ref, sems = refs
        copied([value_ref.at[layer], gate_ref.at[layer]], [pair_ref.at[0], pair_ref.at[1]], sems)
        return
    docs_ref, tokens_ref, pair_ref, tail_ref, sems = refs
    rows, model_width = tokens_ref.shape
    span = round_up(halo, LANES)
    docs = docs_ref[...].reshape(1, rows)[:, rows - span :] + 1
    row = lax.broadcasted_iota(jnp.int32, (LANES, span), 0)
    docs = jnp.where(row == 0, docs // 256, jnp.where(row == 1, docs % 256, 0))
    docs = docs.astype(wide).T[span - halo :, :].astype(narrow)
    part = halo // near
    place = lax.axis_index("tp") % near
    for other in range(near):

        @pl.when(place == other)
        def _(other=other):
            tail_ref[:, model_width:] = docs[other * part : (other + 1) * part, :]

    copied(
        [
            value_ref.at[layer],
            gate_ref.at[layer],
            tokens_ref.at[pl.ds(pl.multiple_of(rows - halo + place * part, HALO_ALIGN), part)],
        ],
        [pair_ref.at[0], pair_ref.at[1], tail_ref.at[:, pl.ds(0, model_width)]],
        sems,
    )


def packed(layer, value_proj, gate_proj, halo=0, near=1, extra=()):
    shapes = [jax.ShapeDtypeStruct((2,) + value_proj.shape[1:], narrow)]
    if halo:
        _, tokens = extra
        shapes.append(jax.ShapeDtypeStruct((halo // near, tokens.shape[1] + LANES), narrow))
    return pl.pallas_call(
        functools.partial(pack_body, layer, halo, near),
        out_shape=tuple(shapes),
        in_specs=[in_hbm()] * 2 + [in_vmem()] * min(1, len(extra)) + [in_hbm()] * (len(extra) - 1),
        out_specs=tuple(in_vmem() for _ in shapes),
        scratch_shapes=[pltpu.SemaphoreType.DMA((3 if halo else 2,))],
        cost_estimate=pl.CostEstimate(flops=PACK_FLOPS, bytes_accessed=PACK_BYTES, transcendentals=0),
        compiler_params=pltpu.CompilerParams(vmem_limit_bytes=KERNEL_VMEM),
    )(value_proj, gate_proj, *extra)


def norm_body(tail, near, tap_count, tokens_ref, docs_ref, gain_ref, *refs):
    prev_refs, refs = refs[:near], refs[near:]
    normed_ref, dist_ref, state_ref, flags_ref, run_ref = refs
    row_count, model_width = tokens_ref.shape
    halo = normed_ref.shape[0] - row_count
    part = halo // near
    rows = halo + row_count
    lead = run_ref.shape[0] - rows
    gain = gain_ref[0:1, :]
    place = lax.axis_index("tp") % near
    for step, prev_ref in enumerate(prev_refs):
        first = pl.multiple_of((place - step + near) % near * part, HALO_ALIGN)
        prev = prev_ref[:, :model_width]
        state_ref[pl.ds(first, part), :] = prev
        normed_ref[pl.ds(first, part), :] = normed_of(prev.astype(wide), gain)
        docs = prev_ref[:, model_width:].astype(wide)
        docs = jnp.broadcast_to(docs[:, 0:1] * 256 + docs[:, 1:2], (part, LANES))
        run_ref[pl.ds(pl.multiple_of(lead + first, SUBLANES), part), :] = docs
    normed_ref[halo:, :] = normed_of(tokens_ref[...].astype(wide), gain)
    own_docs = docs_ref[...].reshape(1, row_count).astype(wide)
    own_docs = jnp.broadcast_to(own_docs, (SUBLANES, row_count)).T[:, 0:1] + 1
    run_ref[:lead, :] = jnp.full((lead, LANES), -1.0, wide)
    run_ref[lead + halo :, :] = jnp.broadcast_to(own_docs, (row_count, LANES))
    same = run_ref[lead:, :] == run_ref[lead - 1 : lead - 1 + rows, :]
    run = jnp.where(same, 1.0, 0.0)
    run_ref[:lead, :] = jnp.zeros((lead, LANES), wide)
    reach = 1
    while reach < tail:
        run_ref[lead:, :] = run
        run = jnp.where(run == reach, reach + run_ref[lead - reach : lead - reach + rows, :], run)
        reach = 2 * reach
    dist_ref[...] = run[tail:, :]
    for k in range(flags_ref.shape[0]):
        least = jnp.min(run[tail + k * CONV_ROWS : tail + (k + 1) * CONV_ROWS, :])
        flags_ref[k] = (least >= tap_count - 1).astype(jnp.int32)


def chunk_start(places, k, size):
    if places is None:
        return 0
    count, steps = places
    return pl.multiple_of(ring_place(count, steps[k]) * size, LANES)


def add_products(acc_ref, start_ref, normed_ref, pairs, places, first_step):
    depth = pairs[0][0].shape[0]
    for k, pair in enumerate(pairs):
        first = chunk_start(places, first_step + k, depth)
        rows_in = normed_ref[:, pl.ds(first, depth)]
        for part in range(2):
            product = jnp.dot(rows_in, pair[part][...], preferred_element_type=wide)
            if k == 0:
                acc_ref[part] = product if start_ref is None else start_ref[part] + product
            else:
                acc_ref[part] += product


def products_body(places, normed_ref, *refs):
    *pair_refs, acc_ref = refs
    pairs = [(pair.at[0], pair.at[1]) for pair in pair_refs]
    add_products(acc_ref, None, normed_ref, pairs, places, 0)


def gated_conv_body(
    layer, tap_count, tail, places, done, halved, flags_ref, normed_ref, dist_ref, taps_ref, *refs
):
    start_ref, refs = (refs[0], refs[1:]) if done else (None, refs)
    *pair_refs, centred_ref, stats_ref, acc_ref, shifted_ref, conv_ref = refs
    pairs = [(pair.at[0], pair.at[1]) for pair in (pair_refs[:-2] if halved else pair_refs)]
    if halved:
        pairs.append(tuple(pair_refs[-2:]))
    width = taps_ref.shape[2]
    halves = width // LANES
    rows = normed_ref.shape[0]
    out_rows = rows - tail
    dist_from = dist_ref.shape[0] - out_rows
    add_products(acc_ref, start_ref, normed_ref, pairs, places, done)
    for half in range(halves):
        cols = slice(half * LANES, (half + 1) * LANES)
        value = acc_ref[0, :, cols].astype(narrow).astype(wide)
        gate = acc_ref[1, :, cols].astype(narrow).astype(wide)
        gated = (value * jax.nn.sigmoid(gate)).astype(narrow).astype(wide)
        shifted_ref[half, 0, :, :] = gated
    for half in range(halves):
        for shift in range(1, SUBLANES):
            shifted_ref[half, shift, SUBLANES:, :] = shifted_ref[
                half, 0, SUBLANES - shift : rows - shift, :
            ]

    def block(index, carry):
        base = pl.multiple_of(index * CONV_ROWS, CONV_ROWS)
        whole = flags_ref[index + dist_from // CONV_ROWS]

        def convolved(masked):
            sums = [jnp.zeros((CONV_ROWS, LANES), wide) for _ in range(halves)]
            if masked:
                dist = dist_ref[pl.ds(pl.multiple_of(base + dist_from, CONV_ROWS), CONV_ROWS), :]
            for tap in range(tap_count):
                start = pl.multiple_of(base + (tail - tap // SUBLANES * SUBLANES), SUBLANES)
                for half in range(halves):
                    term = (
                        taps_ref[tap, layer : layer + 1, half * LANES : (half + 1) * LANES]
                        * shifted_ref[half, tap % SUBLANES, pl.ds(start, CONV_ROWS), :]
                    )
                    sums[half] = sums[half] + (jnp.where(dist >= tap, term, 0.0) if masked else term)
            for half in range(halves):
                conv_ref[half, pl.ds(base, CONV_ROWS), :] = sums[half]

        @pl.when(whole == 1)
        def _():
            convolved(False)

        @pl.when(whole == 0)
        def _():
            convolved(True)

        return carry

    lax.fori_loop(0, out_rows // CONV_ROWS, block, 0)
    total = conv_ref[0]
    for half in range(1, halves):
        total = total + conv_ref[half]
    mean = jnp.sum(total, axis=1, keepdims=True) / width
    square = jnp.zeros((out_rows, LANES), wide)
    for half in range(halves):
        centred = conv_ref[half] - mean
        centred_ref[:, half * LANES : (half + 1) * LANES] = centred.astype(narrow)
        square = square + centred * centred
    square = jnp.sum(square, axis=1, keepdims=True)
    lane = lax.broadcasted_iota(jnp.int32, (out_rows, LANES), 1)
    both = jnp.where(lane == 0, mean, square)
    padded_rows = stats_ref.shape[1]
    if padded_rows != out_rows:
        both = jnp.concatenate([both, jnp.zeros((padded_rows - out_rows, LANES), wide)])
    stats_ref[...] = both.T[:2, :]


def summed(values):
    return functools.reduce(jnp.add, values)


def activate(layer, near, gain_refs, shift_refs, stats_refs, centred_refs, act_ref):
    far = len(centred_refs)
    out_rows, width = centred_refs[0].shape
    count = far * near
    fill = jnp.zeros((round_up(2 * count, SUBLANES) - 2 * count, stats_refs[0].shape[1]), wide)
    stats = jnp.concatenate([ref[...] for ref in stats_refs] + ([fill] if fill.size else []))
    stats = stats.T[:out_rows, :]
    means = [stats[:, 2 * j : 2 * j + 1] for j in range(count)]
    squares = [stats[:, 2 * j + 1 : 2 * j + 2] for j in range(count)]
    mean = summed([summed(means[f * near : (f + 1) * near]) for f in range(far)]) / count
    squares = [square + width * (own - mean) ** 2 for square, own in zip(squares, means)]
    square = summed([summed(squares[f * near : (f + 1) * near]) for f in range(far)])
    scale = lax.rsqrt(square / (width * count) + epsilon)
    for f, centred in enumerate(centred_refs):
        gain, shift = gain_refs[f][layer : layer + 1, :], shift_refs[f][layer : layer + 1, :]
        normal = gain * (centred[...].astype(wide) + (means[f * near] - mean)) * scale + shift
        act_ref[f] = (normal * jax.nn.sigmoid(normal)).astype(narrow)


def project_body(layer, near, far, slots, places, is_first, *refs):
    if is_first:
        gain_refs, shift_refs, refs = refs[:far], refs[far : 2 * far], refs[2 * far :]
        stats_refs, refs = refs[: far * near], refs[far * near :]
        centred_refs, refs = refs[:far], refs[far:]
        *piece_refs, share_ref, act_ref = refs
        activate(layer, near, gain_refs, shift_refs, stats_refs, centred_refs, act_ref)
    else:
        act_ref, *piece_refs, share_ref = refs
    at = 0
    for k in range(len(slots) // far):
        share = None
        for f in range(far):
            piece, slot = piece_refs[k * far + f], slots[k * far + f]
            matrix = piece[...] if slot is None else piece[slot]
            product = jnp.dot(act_ref[f], matrix, preferred_element_type=wide)
            share = product if share is None else share + product
        cols = share.shape[1]
        first = at if places is None else chunk_start(places, k, cols)
        share_ref[:, pl.ds(first, cols)] = share.astype(narrow)
        at = at + cols


def add_body(layer, tail, with_norm, state_count, *refs):
    state_refs, refs = refs[:state_count], refs[state_count:]
    if with_norm:
        gain_ref, *share_refs, hidden_ref, normed_ref = refs
    else:
        *share_refs, hidden_ref = refs
    skip, row = tail, 0
    for state_ref in state_refs:
        from_row = min(skip, state_ref.shape[0])
        skip = skip - from_row
        count = state_ref.shape[0] - from_row
        if count == 0:
            continue
        branch = summed([ref[row : row + count, :].astype(wide) for ref in share_refs])
        state = state_ref[from_row:, :].astype(wide)
        hidden = (state + branch.astype(narrow).astype(wide)).astype(narrow)
        hidden_ref[row : row + count, :] = hidden
        if with_norm:
            gain = gain_ref[layer + 1 : layer + 2, :]
            normed_ref[row : row + count, :] = normed_of(hidden.astype(wide), gain)
        row = row + count


def add_part_body(tail, places, first_step, steps, has_rest, *refs):
    state_ref, *share_refs = refs[: -3 - has_rest]
    hidden_ref, sum_ref, sems = refs[-3:]
    cols = share_refs[0].shape[1] // steps
    copies = []
    for k in range(steps):
        at = slice(k * cols, (k + 1) * cols)
        start = chunk_start(places, first_step + k, cols)
        branch = summed([ref[:, at].astype(wide) for ref in share_refs])
        state = state_ref[tail:, pl.ds(start, cols)].astype(wide)
        sum_ref[:, at] = (state + branch.astype(narrow).astype(wide)).astype(narrow)
        copies.append(
            pltpu.make_async_copy(
                sum_ref.at[:, pl.ds(k * cols, cols)], hidden_ref.at[:, pl.ds(start, cols)], sems.at[k]
            )
        )
        copies[-1].start()
    for copy in copies:
        copy.wait()


def added_part(tail, places, first_step, steps, state, shares, rest, shape):
    return pl.pallas_call(
        functools.partial(add_part_body, tail, places, first_step, steps, len(rest)),
        out_shape=shape,
        in_specs=[in_vmem()] * (1 + len(shares)) + [pl.BlockSpec(memory_space=pl.ANY)] * len(rest),
        out_specs=pl.BlockSpec(memory_space=pl.ANY),
        scratch_shapes=[
            pltpu.VMEM(shares[0].shape, narrow),
            pltpu.SemaphoreType.DMA((steps,)),
        ],
        input_output_aliases={1 + len(shares): 0} if rest else {},
        compiler_params=pltpu.CompilerParams(vmem_limit_bytes=KERNEL_VMEM),
    )(state, *shares, *rest)


def ring_place(count, step):
    index = lax.axis_index("sp")
    odd = index % 2
    position = jnp.where(odd == 1, count - 1 - index // 2, index // 2)
    position = (position + step + count) % count
    return jnp.where(
        position < count // 2, 2 * position, 2 * (count - 1 - position) + 1
    )


def ring_tables(count):
    order = list(range(0, count, 2)) + list(range(count - 1, 0, -2))
    forward = [(order[k], order[(k + 1) % count]) for k in range(count)]
    backward = [(target, source) for source, target in forward]
    steps = [0]
    for k in range(1, count // 2 + 1):
        steps.append(-k)
        if len(steps) < count:
            steps.append(k)
    return forward, backward, steps


def ring_gathered(value):
    count = lax.axis_size("sp")
    forward, backward, _ = ring_tables(count)
    chunks = []
    ahead = behind = value
    for k in range(1, count // 2 + 1):
        if 2 * k == count:
            ahead, behind = ahead[0], behind[1]
        ahead = lax.ppermute(ahead, "sp", forward)
        behind = lax.ppermute(behind, "sp", backward)
        chunks.extend((ahead, behind))
    return chunks


def group_pairs(count, near, far, near_step, far_step):
    pairs = []
    for source in range(count):
        at_far, at_near = source // near, source % near
        target = (at_far + far_step) % far * near + (at_near + near_step) % near
        pairs.append((source, target))
    return pairs


def ringed(sp_count, *widths):
    return sp_count <= RING_MOST and sp_count % 2 == 0 and not any(w % LANES for w in widths)


def tp_groups(tp_count):
    near = 2 if tp_count % 2 == 0 else 1
    return near, tp_count // near


def on_device(
    tokens, doc_ids, pre_gain, value_proj, gate_proj, out_proj, conv_taps, norm_gain, norm_shift
):
    layer_count = value_proj.shape[0]
    tap_count = conv_taps.shape[1]
    row_count, model_width = tokens.shape
    width = conv_taps.shape[2]
    sp_count, tp_count = lax.axis_size("sp"), lax.axis_size("tp")
    near, far = tp_groups(tp_count)
    far_pairs = group_pairs(tp_count, near, far, 0, 1)
    near_pairs = group_pairs(tp_count, near, far, 1, 0)
    tail = round_up(tap_count - 1, max(HALO_ALIGN, CONV_ROWS))
    halo = tail * layer_count
    in_ring = layer_count == 2 and ringed(sp_count, value_proj.shape[1], out_proj.shape[2])

    def far_values(value):
        values = [value]
        for _ in range(1, far):
            values.append(lax.ppermute(values[-1], "tp", far_pairs))
        return values

    docs = doc_ids
    packs = [packed(n, value_proj, gate_proj) for n in range(layer_count - 1)]
    packs.append(packed(layer_count - 1, value_proj, gate_proj, halo, near, (docs, tokens)))
    tail_part = packs[-1][1]
    pair_chunks, out_pieces, out_slots = [], [], []
    if in_ring:
        chunks = [out_proj] + ring_gathered(out_proj)
        chunks = [far_values(chunk) for chunk in chunks]
    for n in range(layer_count):
        pair = packs[n][0]
        if in_ring:
            pair_chunks.append([pair] + ring_gathered(pair))
            pieces = [piece for k in range(len(chunks) - 2) for piece in chunks[k]]
            slots = [n] * len(pieces) + [None] * far
            pieces.extend(chunks[len(chunks) - 2 + n])
        else:
            pair_chunks.append([lax.all_gather(pair, "sp", axis=1, tiled=True)])
            pieces = [
                lax.all_gather(value, "sp", axis=1, tiled=True)
                for value in far_values(out_proj[n])
            ]
            slots = [None] * far
        out_pieces.append(pieces)
        out_slots.append(slots)

    onward = [(source, source + 1) for source in range(sp_count - 1)]
    prev_parts = [lax.ppermute(tail_part, "sp", onward)]
    for _ in range(1, near):
        prev_parts.append(lax.ppermute(prev_parts[-1], "tp", near_pairs))
    gains, shifts = far_values(norm_gain), far_values(norm_shift)
    places = (sp_count, ring_tables(sp_count)[2]) if in_ring else None

    taps = jnp.transpose(conv_taps, (1, 0, 2))
    normed, dist, prev_state, flags = kernel(
        functools.partial(norm_body, tail, near, tap_count),
        (
            jax.ShapeDtypeStruct((halo + row_count, model_width), narrow),
            jax.ShapeDtypeStruct((halo + row_count - tail, LANES), wide),
            jax.ShapeDtypeStruct((halo, model_width), narrow),
            jax.ShapeDtypeStruct(((halo + row_count - tail) // CONV_ROWS,), jnp.int32),
        ),
        [in_vmem()] * (3 + near),
        [pltpu.VMEM((tail + halo + row_count, LANES), wide)],
    )(tokens, docs, pre_gain, *prev_parts)
    states = (prev_state, tokens)

    for n in range(layer_count):
        rows = normed.shape[0]
        out_rows = rows - tail
        pairs = pair_chunks[n]
        done = PRODUCTS_AHEAD[n % 2] if in_ring else 0
        start = ()
        if done:
            start = (
                kernel(
                    functools.partial(products_body, places),
                    jax.ShapeDtypeStruct((2, rows, width), wide),
                    [in_vmem()] * (1 + done),
                )(normed, *pairs[:done]),
            )
        centred, stats = kernel(
            functools.partial(gated_conv_body, n, tap_count, tail, places, done, in_ring),
            (
                jax.ShapeDtypeStruct((out_rows, width), narrow),
                jax.ShapeDtypeStruct((2, round_up(out_rows, LANES)), wide),
            ),
            [in_smem()] + [in_vmem()] * (3 + len(start) + len(pairs) - done),
            [
                pltpu.VMEM((2, rows, width), wide),
                pltpu.VMEM((width // LANES, SUBLANES, rows, LANES), wide),
                pltpu.VMEM((width // LANES, out_rows, LANES), wide),
            ],
        )(flags, normed, dist, taps, *start, *pairs[done:])
        all_stats = [stats]
        for place in range(1, tp_count):
            steps = group_pairs(tp_count, near, far, place % near, place // near)
            all_stats.append(lax.ppermute(stats, "tp", steps))
        pieces = out_pieces[n]
        far_centred = far_values(centred)
        chunk_count = len(pieces) // far
        is_last = n == layer_count - 1
        part_count = SHARE_PARTS if is_last and n > 0 and chunk_count % SHARE_PARTS == 0 else 1
        shares, act = [], ()
        for part in range(part_count):
            own = slice(
                part * chunk_count // part_count * far, (part + 1) * chunk_count // part_count * far
            )
            shape = jax.ShapeDtypeStruct((out_rows, model_width // part_count), narrow)
            act_shape = jax.ShapeDtypeStruct((far, out_rows, width), narrow)
            keeps_act = part_count > 1 and not act
            inputs = act or (*gains, *shifts, *all_stats, *far_centred)
            share, *rest = kernel(
                functools.partial(
                    project_body,
                    n,
                    near,
                    far,
                    out_slots[n][own],
                    places if part_count == 1 else None,
                    not act,
                ),
                (shape,) + ((act_shape,) if keeps_act else ()),
                [in_vmem()] * (len(inputs) + len(pieces[own])),
                [] if act or keeps_act else [pltpu.VMEM(act_shape.shape, narrow)],
            )(*inputs, *pieces[own])
            act = act or tuple(rest)
            shares.append(share)
            for _ in range(1, near):
                shares.append(lax.ppermute(shares[-1], "tp", near_pairs))
        shape = jax.ShapeDtypeStruct((out_rows, model_width), narrow)
        if part_count > 1:
            rest, steps = (), chunk_count // part_count
            for part in range(part_count):
                own = shares[part * near : (part + 1) * near]
                rest = (
                    added_part(tail, places, part * steps, steps, states[0], own, rest, shape),
                )
            return rest[0]
        next_gain = () if is_last else (pre_gain,)
        result = kernel(
            functools.partial(add_body, n, tail, not is_last, len(states)),
            shape if is_last else (shape, shape),
            [in_vmem()] * (len(states) + len(next_gain) + len(shares)),
        )(*states, *next_gain, *shares)
        if is_last:
            return result
        hidden, normed = result
        states = (hidden,)


def solution(mesh):
    return jax.shard_map(
        on_device,
        mesh=mesh,
        in_specs=(
            P("sp", None),
            P("sp"),
            P(),
            P(None, "sp", "tp"),
            P(None, "sp", "tp"),
            P(None, "tp", "sp"),
            P(None, None, "tp"),
            P(None, "tp"),
            P(None, "tp"),
        ),
        out_specs=P("sp", None),
        check_vma=False,
    )
```

```python
import functools

import jax
import jax.numpy as jnp
from jax import lax
from jax.experimental import pallas as pl
from jax.experimental.pallas import tpu as pltpu
from jax.sharding import PartitionSpec as P


epsilon = 1e-06
LANES = 128
SUBLANES = 8
HALO_ALIGN = 16
CONV_MOST = 64
RING_MOST = 8
KERNEL_VMEM = 12 * 2**20
PACK_FLOPS = 2 * 10**9
PACK_BYTES = 8 * 10**6
PRODUCTS_AHEAD = (5, 7)
SHARE_PARTS = 2


wide = jnp.float32
narrow = jnp.bfloat16


def round_up(value, step):
    return -(-value // step) * step


def in_vmem():
    return pl.BlockSpec(memory_space=pltpu.VMEM)


def in_smem():
    return pl.BlockSpec(memory_space=pltpu.SMEM)


def in_hbm():
    return pl.BlockSpec(memory_space=pl.ANY)


def kernel(body, out_shape, in_specs, scratch_shapes=()):
    return pl.pallas_call(
        body,
        out_shape=out_shape,
        in_specs=in_specs,
        out_specs=jax.tree.map(
            lambda shape: in_smem() if len(shape.shape) == 1 else in_vmem(), out_shape
        ),
        scratch_shapes=list(scratch_shapes),
        compiler_params=pltpu.CompilerParams(vmem_limit_bytes=KERNEL_VMEM),
    )


def normed_of(state, gain):
    scale = lax.rsqrt(jnp.mean(state * state, axis=-1, keepdims=True) + epsilon)
    return (state * scale * gain).astype(narrow)


def copied(sources, targets, sems):
    copies = [
        pltpu.make_async_copy(source, target, sems.at[i])
        for i, (source, target) in enumerate(zip(sources, targets))
    ]
    for copy in copies:
        copy.start()
    for copy in copies:
        copy.wait()


def pack_body(layer, halo, near, value_ref, gate_ref, *refs):
    if halo == 0:
        pair_ref, sems = refs
        copied([value_ref.at[layer], gate_ref.at[layer]], [pair_ref.at[0], pair_ref.at[1]], sems)
        return
    docs_ref, tokens_ref, pair_ref, tail_ref, sems = refs
    rows, model_width = tokens_ref.shape
    span = round_up(halo, LANES)
    docs = docs_ref[...].reshape(1, rows)[:, rows - span :] + 1
    row = lax.broadcasted_iota(jnp.int32, (LANES, span), 0)
    docs = jnp.where(row == 0, docs // 256, jnp.where(row == 1, docs % 256, 0))
    docs = docs.astype(wide).T[span - halo :, :].astype(narrow)
    part = halo // near
    place = lax.axis_index("tp") % near
    for other in range(near):

        @pl.when(place == other)
        def _(other=other):
            tail_ref[:, model_width:] = docs[other * part : (other + 1) * part, :]

    copied(
        [
            value_ref.at[layer],
            gate_ref.at[layer],
            tokens_ref.at[pl.ds(pl.multiple_of(rows - halo + place * part, HALO_ALIGN), part)],
        ],
        [pair_ref.at[0], pair_ref.at[1], tail_ref.at[:, pl.ds(0, model_width)]],
        sems,
    )


def packed(layer, value_proj, gate_proj, halo=0, near=1, extra=()):
    shapes = [jax.ShapeDtypeStruct((2,) + value_proj.shape[1:], narrow)]
    if halo:
        _, tokens = extra
        shapes.append(jax.ShapeDtypeStruct((halo // near, tokens.shape[1] + LANES), narrow))
    return pl.pallas_call(
        functools.partial(pack_body, layer, halo, near),
        out_shape=tuple(shapes),
        in_specs=[in_hbm()] * 2 + [in_vmem()] * min(1, len(extra)) + [in_hbm()] * (len(extra) - 1),
        out_specs=tuple(in_vmem() for _ in shapes),
        scratch_shapes=[pltpu.SemaphoreType.DMA((3 if halo else 2,))],
        cost_estimate=pl.CostEstimate(flops=PACK_FLOPS, bytes_accessed=PACK_BYTES, transcendentals=0),
        compiler_params=pltpu.CompilerParams(vmem_limit_bytes=KERNEL_VMEM),
    )(value_proj, gate_proj, *extra)


def norm_body(tail, near, tap_count, blocks, tokens_ref, docs_ref, gain_ref, *refs):
    prev_refs, refs = refs[:near], refs[near:]
    normed_ref, dist_ref, state_ref, flags_ref, run_ref = refs
    row_count, model_width = tokens_ref.shape
    halo = normed_ref.shape[0] - row_count
    part = halo // near
    rows = halo + row_count
    lead = run_ref.shape[0] - rows
    gain = gain_ref[0:1, :]
    place = lax.axis_index("tp") % near
    for step, prev_ref in enumerate(prev_refs):
        first = pl.multiple_of((place - step + near) % near * part, HALO_ALIGN)
        prev = prev_ref[:, :model_width]
        state_ref[pl.ds(first, part), :] = prev
        normed_ref[pl.ds(first, part), :] = normed_of(prev.astype(wide), gain)
        docs = prev_ref[:, model_width:].astype(wide)
        docs = jnp.broadcast_to(docs[:, 0:1] * 256 + docs[:, 1:2], (part, LANES))
        run_ref[pl.ds(pl.multiple_of(lead + first, SUBLANES), part), :] = docs
    normed_ref[halo:, :] = normed_of(tokens_ref[...].astype(wide), gain)
    own_docs = docs_ref[...].reshape(1, row_count).astype(wide)
    own_docs = jnp.broadcast_to(own_docs, (SUBLANES, row_count)).T[:, 0:1] + 1
    run_ref[:lead, :] = jnp.full((lead, LANES), -1.0, wide)
    run_ref[lead + halo :, :] = jnp.broadcast_to(own_docs, (row_count, LANES))
    same = run_ref[lead:, :] == run_ref[lead - 1 : lead - 1 + rows, :]
    run = jnp.where(same, 1.0, 0.0)
    run_ref[:lead, :] = jnp.zeros((lead, LANES), wide)
    reach = 1
    while reach < tail:
        run_ref[lead:, :] = run
        run = jnp.where(run == reach, reach + run_ref[lead - reach : lead - reach + rows, :], run)
        reach = 2 * reach
    dist_ref[...] = run[tail:, :]
    for k, (first, size) in enumerate(blocks):
        flags_ref[k] = (jnp.min(run[first : first + size, :]) >= tap_count - 1).astype(jnp.int32)


def chunk_start(places, k, size):
    if places is None:
        return 0
    count, steps = places
    return pl.multiple_of(ring_place(count, steps[k]) * size, LANES)


def add_products(acc_ref, start_ref, normed_ref, pairs, places, first_step):
    depth = pairs[0][0].shape[0]
    for k, pair in enumerate(pairs):
        first = chunk_start(places, first_step + k, depth)
        rows_in = normed_ref[:, pl.ds(first, depth)]
        for part in range(2):
            product = jnp.dot(rows_in, pair[part][...], preferred_element_type=wide)
            if k == 0:
                acc_ref[part] = product if start_ref is None else start_ref[part] + product
            else:
                acc_ref[part] += product


def products_body(places, normed_ref, *refs):
    *pair_refs, acc_ref = refs
    pairs = [(pair.at[0], pair.at[1]) for pair in pair_refs]
    add_products(acc_ref, None, normed_ref, pairs, places, 0)


def conv_block(rows):
    return max(size for size in range(SUBLANES, CONV_MOST + 1, SUBLANES) if rows % size == 0)


def gated_conv_body(
    layer, tap_count, tail, places, done, halved, flags_from, flags_ref, normed_ref, dist_ref, taps_ref, *refs
):
    start_ref, refs = (refs[0], refs[1:]) if done else (None, refs)
    *pair_refs, centred_ref, stats_ref, acc_ref, shifted_ref, conv_ref = refs
    pairs = [(pair.at[0], pair.at[1]) for pair in (pair_refs[:-2] if halved else pair_refs)]
    if halved:
        pairs.append(tuple(pair_refs[-2:]))
    width = taps_ref.shape[2]
    halves = width // LANES
    rows = normed_ref.shape[0]
    out_rows = rows - tail
    dist_from = dist_ref.shape[0] - out_rows
    add_products(acc_ref, start_ref, normed_ref, pairs, places, done)
    for half in range(halves):
        cols = slice(half * LANES, (half + 1) * LANES)
        value = acc_ref[0, :, cols].astype(narrow).astype(wide)
        gate = acc_ref[1, :, cols].astype(narrow).astype(wide)
        gated = (value * jax.nn.sigmoid(gate)).astype(narrow).astype(wide)
        shifted_ref[half, 0, :, :] = gated
    for half in range(halves):
        for shift in range(1, SUBLANES):
            shifted_ref[half, shift, SUBLANES:, :] = shifted_ref[
                half, 0, SUBLANES - shift : rows - shift, :
            ]

    size = conv_block(out_rows)

    def block(index, carry):
        base = pl.multiple_of(index * size, SUBLANES)
        whole = flags_ref[flags_from + index]

        def convolved(masked):
            if masked:
                dist = dist_ref[pl.ds(pl.multiple_of(base + dist_from, SUBLANES), size), :]
            for half in range(halves):
                cols = slice(half * LANES, (half + 1) * LANES)
                total = jnp.zeros((size, LANES), wide)
                for shift in range(min(SUBLANES, tap_count)):
                    most = (tap_count - 1 - shift) // SUBLANES * SUBLANES
                    start = pl.multiple_of(base + (tail - most), SUBLANES)
                    window = shifted_ref[half, shift, pl.ds(start, size + most), :]
                    for back in range(0, most + 1, SUBLANES):
                        tap = back + shift
                        term = (
                            taps_ref[tap, layer : layer + 1, cols]
                            * window[most - back : most - back + size, :]
                        )
                        total = total + (jnp.where(dist >= tap, term, 0.0) if masked else term)
                conv_ref[half, pl.ds(base, size), :] = total

        @pl.when(whole == 1)
        def _():
            convolved(False)

        @pl.when(whole == 0)
        def _():
            convolved(True)

        return carry

    lax.fori_loop(0, out_rows // size, block, 0)
    total = conv_ref[0]
    for half in range(1, halves):
        total = total + conv_ref[half]
    mean = jnp.sum(total, axis=1, keepdims=True) / width
    square = jnp.zeros((out_rows, LANES), wide)
    for half in range(halves):
        centred = conv_ref[half] - mean
        centred_ref[:, half * LANES : (half + 1) * LANES] = centred.astype(narrow)
        square = square + centred * centred
    square = jnp.sum(square, axis=1, keepdims=True)
    lane = lax.broadcasted_iota(jnp.int32, (out_rows, LANES), 1)
    both = jnp.where(lane == 0, mean, square)
    padded_rows = stats_ref.shape[1]
    if padded_rows != out_rows:
        both = jnp.concatenate([both, jnp.zeros((padded_rows - out_rows, LANES), wide)])
    stats_ref[...] = both.T[:2, :]


def summed(values):
    return functools.reduce(jnp.add, values)


def activate(layer, near, gain_refs, shift_refs, stats_refs, centred_refs, act_ref):
    far = len(centred_refs)
    out_rows, width = centred_refs[0].shape
    count = far * near
    means = [ref[0:1, :] for ref in stats_refs]
    mean = summed([summed(means[f * near : (f + 1) * near]) for f in range(far)]) / count
    squares = [
        ref[1:2, :] + width * (own - mean) ** 2 for ref, own in zip(stats_refs, means)
    ]
    square = summed([summed(squares[f * near : (f + 1) * near]) for f in range(far)])
    lines = [lax.rsqrt(square / (width * count) + epsilon)]
    lines.extend(means[f * near] - mean for f in range(far))
    fill = round_up(len(lines), SUBLANES) - len(lines)
    lines.extend([jnp.zeros_like(mean)] * fill)
    columns = jnp.concatenate(lines).T[:out_rows, :]
    scale = columns[:, 0:1]
    for f, centred in enumerate(centred_refs):
        gain, shift = gain_refs[f][layer : layer + 1, :], shift_refs[f][layer : layer + 1, :]
        offset = columns[:, 1 + f : 2 + f]
        normal = gain * (centred[...].astype(wide) + offset) * scale + shift
        act_ref[f] = (normal * jax.nn.sigmoid(normal)).astype(narrow)


def project_body(layer, near, far, slots, places, is_first, *refs):
    if is_first:
        gain_refs, shift_refs, refs = refs[:far], refs[far : 2 * far], refs[2 * far :]
        stats_refs, refs = refs[: far * near], refs[far * near :]
        centred_refs, refs = refs[:far], refs[far:]
        *piece_refs, share_ref, act_ref = refs
        activate(layer, near, gain_refs, shift_refs, stats_refs, centred_refs, act_ref)
    else:
        act_ref, *piece_refs, share_ref = refs
    at = 0
    for k in range(len(slots) // far):
        share = None
        for f in range(far):
            piece, slot = piece_refs[k * far + f], slots[k * far + f]
            matrix = piece[...] if slot is None else piece[slot]
            product = jnp.dot(act_ref[f], matrix, preferred_element_type=wide)
            share = product if share is None else share + product
        cols = share.shape[1]
        first = at if places is None else chunk_start(places, k, cols)
        share_ref[:, pl.ds(first, cols)] = share.astype(narrow)
        at = at + cols


def add_body(layer, tail, with_norm, state_count, *refs):
    state_refs, refs = refs[:state_count], refs[state_count:]
    if with_norm:
        gain_ref, *share_refs, hidden_ref, normed_ref = refs
    else:
        *share_refs, hidden_ref = refs
    skip, row = tail, 0
    for state_ref in state_refs:
        from_row = min(skip, state_ref.shape[0])
        skip = skip - from_row
        count = state_ref.shape[0] - from_row
        if count == 0:
            continue
        branch = summed([ref[row : row + count, :].astype(wide) for ref in share_refs])
        state = state_ref[from_row:, :].astype(wide)
        hidden = (state + branch.astype(narrow).astype(wide)).astype(narrow)
        hidden_ref[row : row + count, :] = hidden
        if with_norm:
            gain = gain_ref[layer + 1 : layer + 2, :]
            normed_ref[row : row + count, :] = normed_of(hidden.astype(wide), gain)
        row = row + count


def add_part_body(tail, places, first_step, steps, has_rest, *refs):
    state_ref, *share_refs = refs[: -3 - has_rest]
    hidden_ref, sum_ref, sems = refs[-3:]
    cols = share_refs[0].shape[1] // steps
    copies = []
    for k in range(steps):
        at = slice(k * cols, (k + 1) * cols)
        start = chunk_start(places, first_step + k, cols)
        branch = summed([ref[:, at].astype(wide) for ref in share_refs])
        state = state_ref[tail:, pl.ds(start, cols)].astype(wide)
        sum_ref[:, at] = (state + branch.astype(narrow).astype(wide)).astype(narrow)
        copies.append(
            pltpu.make_async_copy(
                sum_ref.at[:, pl.ds(k * cols, cols)], hidden_ref.at[:, pl.ds(start, cols)], sems.at[k]
            )
        )
        copies[-1].start()
    for copy in copies:
        copy.wait()


def added_part(tail, places, first_step, steps, state, shares, rest, shape):
    return pl.pallas_call(
        functools.partial(add_part_body, tail, places, first_step, steps, len(rest)),
        out_shape=shape,
        in_specs=[in_vmem()] * (1 + len(shares)) + [pl.BlockSpec(memory_space=pl.ANY)] * len(rest),
        out_specs=pl.BlockSpec(memory_space=pl.ANY),
        scratch_shapes=[
            pltpu.VMEM(shares[0].shape, narrow),
            pltpu.SemaphoreType.DMA((steps,)),
        ],
        input_output_aliases={1 + len(shares): 0} if rest else {},
        compiler_params=pltpu.CompilerParams(vmem_limit_bytes=KERNEL_VMEM),
    )(state, *shares, *rest)


def ring_place(count, step):
    index = lax.axis_index("sp")
    odd = index % 2
    position = jnp.where(odd == 1, count - 1 - index // 2, index // 2)
    position = (position + step + count) % count
    return jnp.where(
        position < count // 2, 2 * position, 2 * (count - 1 - position) + 1
    )


def ring_tables(count):
    order = list(range(0, count, 2)) + list(range(count - 1, 0, -2))
    forward = [(order[k], order[(k + 1) % count]) for k in range(count)]
    backward = [(target, source) for source, target in forward]
    steps = [0]
    for k in range(1, count // 2 + 1):
        steps.append(-k)
        if len(steps) < count:
            steps.append(k)
    return forward, backward, steps


def ring_gathered(value):
    count = lax.axis_size("sp")
    forward, backward, _ = ring_tables(count)
    chunks = []
    ahead = behind = value
    for k in range(1, count // 2 + 1):
        if 2 * k == count:
            ahead, behind = ahead[0], behind[1]
        ahead = lax.ppermute(ahead, "sp", forward)
        behind = lax.ppermute(behind, "sp", backward)
        chunks.extend((ahead, behind))
    return chunks


def group_pairs(count, near, far, near_step, far_step):
    pairs = []
    for source in range(count):
        at_far, at_near = source // near, source % near
        target = (at_far + far_step) % far * near + (at_near + near_step) % near
        pairs.append((source, target))
    return pairs


def ringed(sp_count, *widths):
    return sp_count <= RING_MOST and sp_count % 2 == 0 and not any(w % LANES for w in widths)


def tp_groups(tp_count):
    near = 2 if tp_count % 2 == 0 else 1
    return near, tp_count // near


def on_device(
    tokens, doc_ids, pre_gain, value_proj, gate_proj, out_proj, conv_taps, norm_gain, norm_shift
):
    layer_count = value_proj.shape[0]
    tap_count = conv_taps.shape[1]
    row_count, model_width = tokens.shape
    width = conv_taps.shape[2]
    sp_count, tp_count = lax.axis_size("sp"), lax.axis_size("tp")
    near, far = tp_groups(tp_count)
    far_pairs = group_pairs(tp_count, near, far, 0, 1)
    near_pairs = group_pairs(tp_count, near, far, 1, 0)
    tail = round_up(tap_count - 1, max(HALO_ALIGN, 2 * HALO_ALIGN))
    halo = tail * layer_count
    in_ring = layer_count == 2 and ringed(sp_count, value_proj.shape[1], out_proj.shape[2])

    def far_values(value):
        values = [value]
        for _ in range(1, far):
            values.append(lax.ppermute(values[-1], "tp", far_pairs))
        return values

    docs = doc_ids
    packs = [packed(n, value_proj, gate_proj) for n in range(layer_count - 1)]
    packs.append(packed(layer_count - 1, value_proj, gate_proj, halo, near, (docs, tokens)))
    tail_part = packs[-1][1]
    pair_chunks, out_pieces, out_slots = [], [], []
    if in_ring:
        chunks = [out_proj] + ring_gathered(out_proj)
        chunks = [far_values(chunk) for chunk in chunks]
    for n in range(layer_count):
        pair = packs[n][0]
        if in_ring:
            pair_chunks.append([pair] + ring_gathered(pair))
            pieces = [piece for k in range(len(chunks) - 2) for piece in chunks[k]]
            slots = [n] * len(pieces) + [None] * far
            pieces.extend(chunks[len(chunks) - 2 + n])
        else:
            pair_chunks.append([lax.all_gather(pair, "sp", axis=1, tiled=True)])
            pieces = [
                lax.all_gather(value, "sp", axis=1, tiled=True)
                for value in far_values(out_proj[n])
            ]
            slots = [None] * far
        out_pieces.append(pieces)
        out_slots.append(slots)

    onward = [(source, source + 1) for source in range(sp_count - 1)]
    prev_parts = [lax.ppermute(tail_part, "sp", onward)]
    for _ in range(1, near):
        prev_parts.append(lax.ppermute(prev_parts[-1], "tp", near_pairs))
    gains, shifts = far_values(norm_gain), far_values(norm_shift)
    places = (sp_count, ring_tables(sp_count)[2]) if in_ring else None

    taps = jnp.transpose(conv_taps, (1, 0, 2))
    blocks, flags_from = [], []
    for n in range(layer_count):
        flags_from.append(len(blocks))
        first = tail * (n + 1)
        size = conv_block(halo + row_count - first)
        blocks.extend((at, size) for at in range(first, halo + row_count, size))
    normed, dist, prev_state, flags = kernel(
        functools.partial(norm_body, tail, near, tap_count, blocks),
        (
            jax.ShapeDtypeStruct((halo + row_count, model_width), narrow),
            jax.ShapeDtypeStruct((halo + row_count - tail, LANES), wide),
            jax.ShapeDtypeStruct((halo, model_width), narrow),
            jax.ShapeDtypeStruct((len(blocks),), jnp.int32),
        ),
        [in_vmem()] * (3 + near),
        [pltpu.VMEM((tail + halo + row_count, LANES), wide)],
    )(tokens, docs, pre_gain, *prev_parts)
    states = (prev_state, tokens)

    for n in range(layer_count):
        rows = normed.shape[0]
        out_rows = rows - tail
        pairs = pair_chunks[n]
        done = PRODUCTS_AHEAD[n % 2] if in_ring else 0
        start = ()
        if done:
            start = (
                kernel(
                    functools.partial(products_body, places),
                    jax.ShapeDtypeStruct((2, rows, width), wide),
                    [in_vmem()] * (1 + done),
                )(normed, *pairs[:done]),
            )
        centred, stats = kernel(
            functools.partial(
                gated_conv_body, n, tap_count, tail, places, done, in_ring, flags_from[n]
            ),
            (
                jax.ShapeDtypeStruct((out_rows, width), narrow),
                jax.ShapeDtypeStruct((2, round_up(out_rows, LANES)), wide),
            ),
            [in_smem()] + [in_vmem()] * (3 + len(start) + len(pairs) - done),
            [
                pltpu.VMEM((2, rows, width), wide),
                pltpu.VMEM((width // LANES, SUBLANES, rows, LANES), wide),
                pltpu.VMEM((width // LANES, out_rows, LANES), wide),
            ],
        )(flags, normed, dist, taps, *start, *pairs[done:])
        all_stats = [stats]
        for place in range(1, tp_count):
            steps = group_pairs(tp_count, near, far, place % near, place // near)
            all_stats.append(lax.ppermute(stats, "tp", steps))
        pieces = out_pieces[n]
        far_centred = far_values(centred)
        chunk_count = len(pieces) // far
        is_last = n == layer_count - 1
        part_count = SHARE_PARTS if is_last and n > 0 and chunk_count % SHARE_PARTS == 0 else 1
        shares, act = [], ()
        for part in range(part_count):
            own = slice(
                part * chunk_count // part_count * far, (part + 1) * chunk_count // part_count * far
            )
            shape = jax.ShapeDtypeStruct((out_rows, model_width // part_count), narrow)
            act_shape = jax.ShapeDtypeStruct((far, out_rows, width), narrow)
            keeps_act = part_count > 1 and not act
            inputs = act or (*gains, *shifts, *all_stats, *far_centred)
            share, *rest = kernel(
                functools.partial(
                    project_body,
                    n,
                    near,
                    far,
                    out_slots[n][own],
                    places if part_count == 1 else None,
                    not act,
                ),
                (shape,) + ((act_shape,) if keeps_act else ()),
                [in_vmem()] * (len(inputs) + len(pieces[own])),
                [] if act or keeps_act else [pltpu.VMEM(act_shape.shape, narrow)],
            )(*inputs, *pieces[own])
            act = act or tuple(rest)
            shares.append(share)
            for _ in range(1, near):
                shares.append(lax.ppermute(shares[-1], "tp", near_pairs))
        shape = jax.ShapeDtypeStruct((out_rows, model_width), narrow)
        if part_count > 1:
            rest, steps = (), chunk_count // part_count
            for part in range(part_count):
                own = shares[part * near : (part + 1) * near]
                rest = (
                    added_part(tail, places, part * steps, steps, states[0], own, rest, shape),
                )
            return rest[0]
        next_gain = () if is_last else (pre_gain,)
        result = kernel(
            functools.partial(add_body, n, tail, not is_last, len(states)),
            shape if is_last else (shape, shape),
            [in_vmem()] * (len(states) + len(next_gain) + len(shares)),
        )(*states, *next_gain, *shares)
        if is_last:
            return result
        hidden, normed = result
        states = (hidden,)


def solution(mesh):
    return jax.shard_map(
        on_device,
        mesh=mesh,
        in_specs=(
            P("sp", None),
            P("sp"),
            P(),
            P(None, "sp", "tp"),
            P(None, "sp", "tp"),
            P(None, "tp", "sp"),
            P(None, None, "tp"),
            P(None, "tp"),
            P(None, "tp"),
        ),
        out_specs=P("sp", None),
        check_vma=False,
    )
```
